32 devices in a mesh: grp: 2 (over y), sp: 4 (over z), tp: 4 (over x, core).
Axes of the slice: x: 2, y: 2, z: 4, core: 2. Of those that a mesh axis runs over, the one named last changes fastest.
Arguments:
- recurrent_query: bfloat16 [2048, 1024], P(('grp', 'sp'), 'tp'), parts along dimension 0, may hold values from -6 to 6
- recurrent_forget_gate: bfloat16 [2048, 1024], P(('grp', 'sp'), 'tp'), parts along dimension 0, may hold values from -4.5 to 4.5
- recurrent_value: bfloat16 [2048, 1024], P(('grp', 'sp'), 'tp'), parts along dimension 0, may hold values from -6 to 6
- recurrent_gate_lower_bound: float32 [1024], P('tp'), may hold values from 1.5 to 14
- recurrent_added_decay: float32 [2048, 8], P(('grp', 'sp'), 'tp'), parts along dimension 0, may hold values from -0.51 to 0
- recurrent_norm_gain: float32 [128], replicated, may hold values from 0.1 to 1.9
- attention_query_first: bfloat16 [2048, 512], P(('grp', 'sp'), 'tp'), parts along dimension 0, may hold values from -20 to 20
- attention_key_first: bfloat16 [2048, 256], P(('grp', 'sp'), 'tp'), parts along dimension 0, may hold values from -20 to 20
- attention_query_second: bfloat16 [2048, 512], P(('grp', 'sp'), 'tp'), parts along dimension 0, may hold values from -20 to 20
- attention_key_second: bfloat16 [2048, 256], P(('grp', 'sp'), 'tp'), parts along dimension 0, may hold values from -20 to 20
- attention_value: bfloat16 [2048, 512], P(('grp', 'sp'), 'tp'), parts along dimension 0, may hold values from -6 to 6
- second_map_weight: float32 [8], P('tp'), may hold values from 0.3 to 0.8
- attention_norm_gain: float32 [128], replicated, may hold values from 0.1 to 1.9
- output_weight: bfloat16 [2, 1024, 2048], P(None, 'tp', 'sp'), may hold values from -0.125 to 0.125
Outputs:
- mixed: bfloat16 [2048, 2048], P(('grp', 'sp', 'tp')), parts along dimension 0
The draws below stay inside these ranges and needn't reach their ends.
There are 2 independent parts, one for each index of `grp`. The reference program is written for one: setup_inputs(seed, part) draws one part's arguments, and reference() takes and returns one part's arrays. A program takes and returns all parts, laid end to end along the dimension named above; an argument that names none is the same for every part. Nothing has to cross between parts.
All inputs are finite; a program needn't handle non-finite values.
Results may differ from the reference program's by a relative error of at most 0.02.
Values may be sent and summed in bfloat16 or wider, within the bound.
No kernel may reach another device: no remote copies, remote signals or barrier semaphores. Data moves between devices by JAX's collectives and lax.ppermute only.
A program may use at most 64 MiB of HBM per device.

```python
import jax
import jax.numpy as jnp
from jax import lax

D = 2048
RECURRENT_HEADS = 8
HG_DK = 128
HG_DV = 128
DA_HEADS = 8
KV_HEADS = 4
DA_HD = 64
BLK = 32
TOK_DEV = 256
TOKENS = 1024
MIX_WIDTH = 1024
N_TP = 4


def loguniform_draw(key, shape, low, high):
    return jnp.exp(jax.random.uniform(key, shape, jnp.float32, jnp.log(low), jnp.log(high)))


def draw_recurrent_gate_lower_bound(key, part):
    split_keys = jax.random.split(key, 4)
    order = jax.random.permutation(split_keys[0], RECURRENT_HEADS)
    fast = order < RECURRENT_HEADS // 2
    fast_rate = loguniform_draw(split_keys[1], (RECURRENT_HEADS,), 0.04, 0.12)
    slow_rate = loguniform_draw(split_keys[2], (RECURRENT_HEADS,), 0.3, 1.2) / TOKENS
    jitter = loguniform_draw(split_keys[3], (RECURRENT_HEADS, HG_DK), 0.7, 1.4)
    floor_rate = jnp.where(fast, fast_rate, slow_rate)[:, None] * jitter
    return jnp.log(1.0 / floor_rate - 1.0).reshape(-1).astype(jnp.float32)


def draw_recurrent_forget_gate(key, part):
    split_keys = jax.random.split(key, 2)
    block_count = TOKENS // TOK_DEV
    shift = jax.random.uniform(split_keys[0], (block_count, 1, RECURRENT_HEADS, 1), jnp.float32, -1.5, 1.5)
    rough = jax.random.truncated_normal(split_keys[1], -3.0, 3.0, (block_count, TOK_DEV, RECURRENT_HEADS, HG_DK), jnp.float32)
    return (rough + shift).reshape(TOKENS, RECURRENT_HEADS * HG_DK).astype(jnp.bfloat16)


def draw_recurrent_added_decay(key, part):
    split_keys = jax.random.split(key, 2)
    spots = jax.random.randint(split_keys[0], (3, RECURRENT_HEADS), 0, TOKENS)
    depth = jax.random.uniform(split_keys[1], (3, RECURRENT_HEADS), jnp.float32, -0.51, -0.22)
    matches = jnp.arange(TOKENS)[:, None, None] == spots[None]
    return jnp.min(jnp.where(matches, depth[None], 0.0), axis=1).astype(jnp.float32)


def draw_pair(key, marker):
    base = jax.random.fold_in(key, marker)
    split_keys = jax.random.split(base, 2)
    queries = 1.3 * jax.random.truncated_normal(split_keys[0], -6.0, 6.0, (TOKENS, DA_HEADS * DA_HD), jnp.float32)
    key_rows = 1.3 * jax.random.truncated_normal(split_keys[1], -6.0, 6.0, (TOKENS, KV_HEADS * DA_HD), jnp.float32)
    return (queries.astype(jnp.bfloat16), key_rows.astype(jnp.bfloat16))


def draw_attention_query_first(key, part):
    return draw_pair(key, 11)[0]


def draw_attention_key_first(key, part):
    return draw_pair(key, 11)[1]


def draw_attention_query_second(key, part):
    return draw_pair(key, 12)[0]


def draw_attention_key_second(key, part):
    return draw_pair(key, 12)[1]


def shard_levels(stream_key, shape, pieces, smallest, high):
    def one(axis_at, shards_of):
        draws = jax.random.uniform(jax.random.fold_in(jax.random.fold_in(stream_key, 6), axis_at), (shards_of,), jnp.float32, smallest / len(pieces), high / len(pieces))
        return jnp.repeat(jnp.exp(draws), shape[axis_at] // shards_of).reshape((-1,) + (1,) * (len(shape) - axis_at - 1))

    loudness = one(*pieces[0])
    for cut in pieces[1:]:
        loudness = loudness * one(*cut)
    return loudness


def scatter_about(rng, extent, width, most, cuts=(), held_as=jnp.bfloat16):
    loudness = shard_levels(rng, extent, cuts, -0.22, 0.18) if cuts else 1.0
    array = jax.random.normal(rng, extent, jnp.float32) * width * loudness
    return jnp.minimum(jnp.maximum(array, -most), most).astype(held_as)


def setup_inputs(seed: int = 0, part: int = 0) -> dict:
    keys = jax.random.split(jax.random.key(seed), 15)
    own_keys = jax.random.split(jax.random.fold_in(keys[14], part), 15)
    recurrent_query = scatter_about(own_keys[0], (TOKENS, RECURRENT_HEADS * HG_DK), 1.0, 6.0, ((0, 4), (1, 4)))
    recurrent_forget_gate = draw_recurrent_forget_gate(jax.random.fold_in(jax.random.fold_in(keys[14], part), 71), part)
    recurrent_value = scatter_about(own_keys[2], (TOKENS, MIX_WIDTH), 1.0, 6.0, ((0, 4), (1, 4)))
    recurrent_gate_lower_bound = draw_recurrent_gate_lower_bound(jax.random.fold_in(keys[14], 71), part)
    recurrent_added_decay = draw_recurrent_added_decay(jax.random.fold_in(jax.random.fold_in(keys[14], part), 71), part)
    recurrent_norm_gain = jnp.clip(1.0 + 0.18 * jax.random.normal(keys[5], (HG_DV,), jnp.float32), 0.1, 1.9)
    attention_query_first = draw_attention_query_first(jax.random.fold_in(jax.random.fold_in(keys[14], part), 71), part)
    attention_key_first = draw_attention_key_first(jax.random.fold_in(jax.random.fold_in(keys[14], part), 71), part)
    attention_query_second = draw_attention_query_second(jax.random.fold_in(jax.random.fold_in(keys[14], part), 71), part)
    attention_key_second = draw_attention_key_second(jax.random.fold_in(jax.random.fold_in(keys[14], part), 71), part)
    attention_value = scatter_about(own_keys[10], (TOKENS, KV_HEADS * 2 * DA_HD), 1.0, 6.0, ((0, 4), (1, 4)))
    second_map_weight = jnp.clip(0.3 + 0.5 * jax.random.uniform(keys[11], (DA_HEADS,), jnp.float32) ** shard_levels(keys[11], (DA_HEADS,), ((0, 4),), -0.2, 0.2), 0.3, 0.8)
    attention_norm_gain = jnp.clip(1.0 + 0.18 * jax.random.normal(keys[12], (2 * DA_HD,), jnp.float32), 0.1, 1.9)
    output_weight = scatter_about(keys[13], (2, MIX_WIDTH, D), (2 * MIX_WIDTH) ** -0.5, 0.125, ((1, 4), (2, 4)))
    return dict(recurrent_query=recurrent_query, recurrent_forget_gate=recurrent_forget_gate, recurrent_value=recurrent_value, recurrent_gate_lower_bound=recurrent_gate_lower_bound, recurrent_added_decay=recurrent_added_decay, recurrent_norm_gain=recurrent_norm_gain, attention_query_first=attention_query_first, attention_key_first=attention_key_first, attention_query_second=attention_query_second, attention_key_second=attention_key_second, attention_value=attention_value, second_map_weight=second_map_weight, attention_norm_gain=attention_norm_gain, output_weight=output_weight)


epsilon = 1e-06
highest = lax.Precision.HIGHEST

def head_norm(head_values, gain_vec):
    mean_square = lax.optimization_barrier(jnp.mean(head_values * head_values, axis=-1, keepdims=True))
    return head_values * lax.rsqrt(mean_square + epsilon) * gain_vec

def decay_factors(gate_preactivation, lower_bound_logit, added_log_decay, number_of_heads):
    token_count = gate_preactivation.shape[0]
    floor_rate = jax.nn.sigmoid(-lower_bound_logit).reshape(number_of_heads, -1)
    state_inflow = floor_rate[None] * jax.nn.sigmoid(-gate_preactivation.astype(jnp.float32)).reshape(token_count, number_of_heads, -1)
    decay_logarithm = jnp.log1p(-state_inflow) + added_log_decay[:, :, None]
    return (state_inflow, decay_logarithm)

def recurrence_blocks(queries, decay_logarithm, state_inflow, value_rows, block_len):
    token_count, number_of_heads, key_width = queries.shape
    block_count = token_count // block_len

    def to_blocks(source):
        return source.reshape(block_count, block_len, number_of_heads, source.shape[-1])
    causal = jnp.tril(jnp.ones((block_len, block_len), jnp.float32))[:, :, None, None]

    def block_step(carry_state, inputs):
        query_blk, decay_blk, inflow_blk, value_blk = inputs
        cumulative = jnp.cumsum(decay_blk, axis=0)
        relative = cumulative[:, None] - cumulative[None, :]
        decay_table = jnp.exp(jnp.minimum(relative, 0.0)) * causal
        scores = jnp.einsum('thd,shd,tshd->hts', query_blk, inflow_blk, decay_table, precision=highest)
        block_out = jnp.einsum('hts,shv->thv', scores, value_blk, precision=highest)
        block_out = block_out + jnp.einsum('thd,hdv->thv', query_blk * jnp.exp(cumulative), carry_state, precision=highest)
        last_log = cumulative[-1]
        new_state = jnp.exp(last_log)[:, :, None] * carry_state + jnp.einsum('shd,shv->hdv', inflow_blk * jnp.exp(last_log[None] - cumulative), value_blk, precision=highest)
        return (new_state, block_out)
    zero_state = jnp.zeros((number_of_heads, key_width, value_rows.shape[-1]), jnp.float32)
    final_state, outputs = lax.scan(block_step, zero_state, (to_blocks(queries), to_blocks(decay_logarithm), to_blocks(state_inflow), to_blocks(value_rows)))
    return (final_state, outputs.reshape(token_count, number_of_heads, -1))

def recurrent_token_mixer(recurrent_query, recurrent_forget_gate, recurrent_value, recurrent_gate_lower_bound, recurrent_added_decay, recurrent_norm_gain):
    token_count = recurrent_query.shape[0]
    state_inflow, decay_logarithm = decay_factors(recurrent_forget_gate, recurrent_gate_lower_bound, recurrent_added_decay, RECURRENT_HEADS)
    queries = recurrent_query.astype(jnp.float32).reshape(token_count, RECURRENT_HEADS, HG_DK)
    value_rows = recurrent_value.astype(jnp.float32).reshape(token_count, RECURRENT_HEADS, HG_DV)
    unused, mixed_rows = recurrence_blocks(queries, decay_logarithm, state_inflow, value_rows, BLK)
    return head_norm(mixed_rows, recurrent_norm_gain).astype(jnp.bfloat16)

def difference_mixer(attention_query_first, attention_key_first, attention_query_second, attention_key_second, attention_value, second_map_weight, attention_norm_gain):
    token_count = attention_query_first.shape[0]
    group_size = DA_HEADS // KV_HEADS
    score_scale = DA_HD ** (-0.5)
    keys_one = attention_key_first.astype(jnp.float32).reshape(token_count, KV_HEADS, DA_HD)
    keys_two = attention_key_second.astype(jnp.float32).reshape(token_count, KV_HEADS, DA_HD)
    value_rows = attention_value.astype(jnp.float32).reshape(token_count, KV_HEADS, 2 * DA_HD)
    lambda_table = second_map_weight.reshape(KV_HEADS, group_size)
    key_pos = jnp.arange(token_count).astype(jnp.int32)

    def per_block(block_index):
        first_row = (block_index * TOK_DEV).astype(jnp.int32)
        query_pos = first_row + jnp.arange(TOK_DEV).astype(jnp.int32)
        allowed = key_pos[None, :] <= query_pos[:, None]

        def slice_queries(source):
            picked = lax.dynamic_slice_in_dim(source, first_row, TOK_DEV, 0)
            return picked.astype(jnp.float32).reshape(TOK_DEV, KV_HEADS, group_size, DA_HD)
        queries_one = slice_queries(attention_query_first)
        queries_two = slice_queries(attention_query_second)

        def per_head(head_index):
            results = []
            for queries, key_rows in ((queries_one, keys_one), (queries_two, keys_two)):
                scores = jnp.einsum('qgd,sd->gqs', queries[:, head_index], key_rows[:, head_index], precision=highest) * score_scale
                scores = jnp.where(allowed[None], scores, -1e+30)
                row_max = lax.optimization_barrier(jnp.max(scores, axis=-1, keepdims=True))
                weights = jnp.where(allowed[None], jnp.exp(scores - row_max), 0.0)
                weight_mass = lax.optimization_barrier(jnp.sum(weights, axis=-1))
                rounded = lax.optimization_barrier(weights.astype(jnp.bfloat16)).astype(jnp.float32)
                product = jnp.einsum('gqs,sv->gqv', rounded, value_rows[:, head_index], precision=highest)
                results.append(product / weight_mass[..., None])
            return results[0] - lambda_table[head_index][:, None, None] * results[1]
        heads_out = lax.map(per_head, jnp.arange(KV_HEADS).astype(jnp.int32))
        return jnp.transpose(heads_out, (2, 0, 1, 3)).reshape(TOK_DEV, DA_HEADS, 2 * DA_HD)
    blocks = lax.map(per_block, jnp.arange(token_count // TOK_DEV).astype(jnp.int32))
    mixed_rows = blocks.reshape(token_count, DA_HEADS, 2 * DA_HD)
    return head_norm(mixed_rows, attention_norm_gain).astype(jnp.bfloat16)

def reference(recurrent_query, recurrent_forget_gate, recurrent_value, recurrent_gate_lower_bound, recurrent_added_decay, recurrent_norm_gain, attention_query_first, attention_key_first, attention_query_second, attention_key_second, attention_value, second_map_weight, attention_norm_gain, output_weight):
    recurrent_output = recurrent_token_mixer(recurrent_query, recurrent_forget_gate, recurrent_value, recurrent_gate_lower_bound, recurrent_added_decay, recurrent_norm_gain)
    attended = difference_mixer(attention_query_first, attention_key_first, attention_query_second, attention_key_second, attention_value, second_map_weight, attention_norm_gain)
    token_count = recurrent_query.shape[0]
    rec_share = RECURRENT_HEADS // N_TP
    att_share = DA_HEADS // N_TP
    row_share = MIX_WIDTH // N_TP
    summed = jnp.zeros((token_count, D), jnp.float32)
    for member in range(N_TP):
        rec_part = recurrent_output[:, member * rec_share:(member + 1) * rec_share].reshape(token_count, -1)
        att_part = attended[:, member * att_share:(member + 1) * att_share].reshape(token_count, -1)
        rows_rec = output_weight[0, member * row_share:(member + 1) * row_share]
        rows_att = output_weight[1, member * row_share:(member + 1) * row_share]
        partial_term = jnp.dot(rec_part, rows_rec, preferred_element_type=jnp.float32) + jnp.dot(att_part, rows_att, preferred_element_type=jnp.float32)
        summed = summed + lax.optimization_barrier(partial_term.astype(jnp.bfloat16)).astype(jnp.float32)
    return summed.astype(jnp.bfloat16)
```

```python
import functools

import jax
import jax.numpy as jnp
from jax import lax
from jax.experimental import pallas as pl
from jax.experimental.pallas import tpu as pltpu
from jax.sharding import PartitionSpec as P

HG_DK = 128
HG_DV = 128
DA_HD = 64
BLK = 32


epsilon = 1e-06
highest = lax.Precision.HIGHEST
key_span = 512


def carried_in(array, axis, combine, identity):
    size, place = (lax.axis_size(axis), lax.axis_index(axis))
    everything = jax.tree.map(
        lambda part, kind: lax.all_gather(part.astype(kind), axis),
        array,
        (jnp.bfloat16, jnp.bfloat16),
    )
    start = jax.tree.map(
        lambda part, zero: jnp.broadcast_to(jnp.asarray(zero, part.dtype), part.shape),
        array,
        identity,
    )

    def hop(k, before):
        reached = k < place
        new = combine(
            before, jax.tree.map(lambda part, own: part[k].astype(own.dtype), everything, array)
        )
        return jax.tree.map(lambda a, b: jnp.where(reached, a, b), new, before)

    return lax.fori_loop(0, size, hop, start)


def head_norm(head_values, gain_vec):
    mean_square = jnp.mean(head_values * head_values, axis=-1, keepdims=True)
    return head_values * lax.rsqrt(mean_square + epsilon) * gain_vec


def decay_factors(gate_preactivation, lower_bound_logit, added_log_decay, number_of_heads):
    token_count = gate_preactivation.shape[0]
    floor_rate = jax.nn.sigmoid(-lower_bound_logit).reshape(number_of_heads, -1)
    state_inflow = floor_rate[None] * jax.nn.sigmoid(
        -gate_preactivation.astype(jnp.float32)
    ).reshape(token_count, number_of_heads, -1)
    decay_logarithm = jnp.log1p(-state_inflow) + added_log_decay[:, :, None]
    return (state_inflow, decay_logarithm)


def recurrence_blocks(queries, decay_logarithm, state_inflow, value_rows, block_len):
    token_count, number_of_heads, key_width = queries.shape
    block_count = token_count // block_len

    def to_blocks(source):
        return source.reshape(block_count, block_len, number_of_heads, source.shape[-1])

    causal = jnp.tril(jnp.ones((block_len, block_len), jnp.float32))[:, :, None, None]

    def block_step(carry_state, inputs):
        query_blk, decay_blk, inflow_blk, value_blk = inputs
        cumulative = jnp.cumsum(decay_blk, axis=0)
        relative = cumulative[:, None] - cumulative[None, :]
        decay_table = jnp.exp(jnp.minimum(relative, 0.0)) * causal
        scores = jnp.einsum(
            "thd,shd,tshd->hts", query_blk, inflow_blk, decay_table, precision=highest
        )
        block_out = jnp.einsum("hts,shv->thv", scores, value_blk, precision=highest)
        block_out = block_out + jnp.einsum(
            "thd,hdv->thv", query_blk * jnp.exp(cumulative), carry_state, precision=highest
        )
        last_log = cumulative[-1]
        new_state = jnp.exp(last_log)[:, :, None] * carry_state + jnp.einsum(
            "shd,shv->hdv",
            inflow_blk * jnp.exp(last_log[None] - cumulative),
            value_blk,
            precision=highest,
        )
        return (new_state, block_out)

    zero_state = jnp.zeros((number_of_heads, key_width, value_rows.shape[-1]), jnp.float32)
    final_state, outputs = lax.scan(
        block_step,
        zero_state,
        (
            to_blocks(queries),
            to_blocks(decay_logarithm),
            to_blocks(state_inflow),
            to_blocks(value_rows),
        ),
    )
    return (final_state, outputs.reshape(token_count, number_of_heads, -1))


def chain_pair(earlier, following):
    return (earlier[0] * following[0], following[0][:, :, None] * earlier[1] + following[1])


def recurrent_path_output(
    recurrent_query,
    recurrent_forget_gate,
    recurrent_value,
    recurrent_gate_lower_bound,
    recurrent_added_decay,
    recurrent_norm_gain,
):
    token_count = recurrent_query.shape[0]
    number_of_heads = recurrent_gate_lower_bound.shape[0] // HG_DK
    state_inflow, decay_logarithm = decay_factors(
        recurrent_forget_gate, recurrent_gate_lower_bound, recurrent_added_decay, number_of_heads
    )
    queries = recurrent_query.astype(jnp.float32).reshape(token_count, number_of_heads, HG_DK)
    value_rows = recurrent_value.astype(jnp.float32).reshape(token_count, number_of_heads, HG_DV)
    final_state, local_out = recurrence_blocks(
        queries, decay_logarithm, state_inflow, value_rows, BLK
    )
    running_log = jnp.cumsum(decay_logarithm, axis=0)
    through = jnp.exp(running_log[-1])
    incoming = carried_in(
        (through, final_state),
        "sp",
        chain_pair,
        (jnp.ones_like(through), jnp.zeros_like(final_state)),
    )
    carried = jnp.einsum(
        "thd,hdv->thv", queries * jnp.exp(running_log), incoming[1], precision=highest
    )
    return (
        head_norm(local_out + carried, recurrent_norm_gain)
        .astype(jnp.bfloat16)
        .reshape(token_count, -1)
    )


def attention_branch(
    attention_query_first,
    attention_key_first,
    attention_query_second,
    attention_key_second,
    attention_value,
    second_map_weight,
    attention_norm_gain,
):
    query_rows = attention_query_first.shape[0]
    key_heads = attention_key_first.shape[1] // DA_HD
    group_size = attention_query_first.shape[1] // DA_HD // key_heads
    score_scale = DA_HD ** (-0.5)
    offset = lax.axis_index("sp") * query_rows
    query_pos = offset + jnp.arange(query_rows)
    last_query = offset + query_rows - 1
    queries_one = attention_query_first.reshape(query_rows, key_heads, group_size, DA_HD)
    queries_two = attention_query_second.reshape(query_rows, key_heads, group_size, DA_HD)

    def map_update(running, queries, key_rows, value_rows, allowed):
        row_max, weight_mass, value_sum = running
        scores = (
            jnp.einsum("qkgd,skd->kgqs", queries, key_rows, preferred_element_type=jnp.float32)
            * score_scale
        )
        scores = jnp.where(allowed, scores, -1e30)
        new_max = jnp.maximum(row_max, jnp.max(scores, axis=-1))
        weights = jnp.where(allowed, jnp.exp(scores - new_max[..., None]), 0.0)
        shrink = jnp.exp(row_max - new_max)
        weight_mass = weight_mass * shrink + jnp.sum(weights, axis=-1)
        value_sum = value_sum * shrink[..., None] + jnp.einsum(
            "plew,wpd->pled",
            weights.astype(jnp.bfloat16),
            value_rows,
            preferred_element_type=jnp.float32,
        )
        return (new_max, weight_mass, value_sum)

    def key_block(running, block_one, block_two, block_values, first_row):
        span_rows = block_one.shape[0]
        key_pos = first_row + jnp.arange(span_rows)
        allowed = key_pos[None, :] <= query_pos[:, None]
        shaped_one = block_one.reshape(span_rows, key_heads, DA_HD)
        shaped_two = block_two.reshape(span_rows, key_heads, DA_HD)
        shaped_values = block_values.reshape(span_rows, key_heads, 2 * DA_HD)
        return (
            map_update(running[0], queries_one, shaped_one, shaped_values, allowed),
            map_update(running[1], queries_two, shaped_two, shaped_values, allowed),
        )

    def guarded_block(running, block_one, block_two, block_values, first_row):

        def compute(state_in):
            return key_block(state_in, block_one, block_two, block_values, first_row)

        def unchanged(state_in):
            return state_in

        result = lax.cond(first_row > last_query, unchanged, compute, running)
        return result

    start_max = jnp.full((key_heads, group_size, query_rows), -1e30, jnp.float32)
    zero_mass = jnp.zeros((key_heads, group_size, query_rows), jnp.float32)
    zero_sum = jnp.zeros((key_heads, group_size, query_rows, 2 * DA_HD), jnp.float32)
    fresh_state = (start_max, zero_mass, zero_sum)
    running = (fresh_state, fresh_state)
    shard_one = lax.all_gather(attention_key_first, "sp", axis=0, tiled=True)
    shard_two = lax.all_gather(attention_key_second, "sp", axis=0, tiled=True)
    shard_values = lax.all_gather(attention_value, "sp", axis=0, tiled=True)
    row_count = shard_one.shape[0]
    span_rows = min(row_count, key_span)
    full_count = row_count // span_rows

    def span_step(span_index, state_in):
        begin_row = span_index * span_rows
        return guarded_block(
            state_in,
            lax.dynamic_slice_in_dim(shard_one, begin_row, span_rows, 0),
            lax.dynamic_slice_in_dim(shard_two, begin_row, span_rows, 0),
            lax.dynamic_slice_in_dim(shard_values, begin_row, span_rows, 0),
            begin_row,
        )

    running = lax.fori_loop(0, full_count, span_step, running)
    first_map, second_map = running
    lambda_table = second_map_weight.reshape(key_heads, group_size)[:, :, None, None]
    combined = first_map[2] / first_map[1][..., None] - lambda_table * (
        second_map[2] / second_map[1][..., None]
    )
    combined = jnp.transpose(combined, (2, 0, 1, 3)).reshape(
        query_rows, key_heads * group_size, 2 * DA_HD
    )
    return head_norm(combined, attention_norm_gain).astype(jnp.bfloat16).reshape(query_rows, -1)


def general_shards(
    recurrent_query,
    recurrent_forget_gate,
    recurrent_value,
    recurrent_gate_lower_bound,
    recurrent_added_decay,
    recurrent_norm_gain,
    attention_query_first,
    attention_key_first,
    attention_query_second,
    attention_key_second,
    attention_value,
    second_map_weight,
    attention_norm_gain,
    output_weight,
):
    attended = attention_branch(
        attention_query_first,
        attention_key_first,
        attention_query_second,
        attention_key_second,
        attention_value,
        second_map_weight,
        attention_norm_gain,
    )
    recurrent_output = recurrent_path_output(
        recurrent_query,
        recurrent_forget_gate,
        recurrent_value,
        recurrent_gate_lower_bound,
        recurrent_added_decay,
        recurrent_norm_gain,
    )
    pieces = lax.all_gather(output_weight, "sp", axis=2, tiled=True)
    partial_terms = jnp.dot(
        recurrent_output, pieces[0], preferred_element_type=jnp.float32
    ) + jnp.dot(attended, pieces[1], preferred_element_type=jnp.float32)
    return lax.psum_scatter(
        partial_terms.astype(jnp.bfloat16), "tp", scatter_dimension=0, tiled=True
    )


f32 = jnp.float32
bf16 = jnp.bfloat16
SPARE_ROWS = 16


def dot_nt(a, b):
    return lax.dot_general(a, b, (((1,), (1,)), ((), ())), preferred_element_type=f32)


def dot_nn(a, b):
    return jnp.dot(a, b, preferred_element_type=f32)


def dot_tn(a, b):
    return lax.dot_general(a, b, (((0,), (0,)), ((), ())), preferred_element_type=f32)


def cost(flops, *arrays):
    moved = sum(a.size * a.dtype.itemsize for a in arrays)
    return pl.CostEstimate(flops=flops, bytes_accessed=moved, transcendentals=0)


def recurrence_kernel(
    query_ref, gate_ref, value_ref, bound_ref, added_ref, local_ref, faded_ref, state_ref
):
    token_count, width = query_ref.shape
    heads = width // HG_DK
    chunk = min(token_count, HG_DK)
    floor_rate = jax.nn.sigmoid(-bound_ref[...])
    inflow = floor_rate * jax.nn.sigmoid(-gate_ref[...].astype(f32))
    added = added_ref[...]
    wide = [jnp.broadcast_to(added[:, h : h + 1], (token_count, HG_DK)) for h in range(heads)]
    log_decay = jnp.log1p(-inflow) + jnp.concatenate(wide, axis=1)
    row = lax.broadcasted_iota(jnp.int32, (chunk, chunk), 0)
    column = lax.broadcasted_iota(jnp.int32, (chunk, chunk), 1)
    causal = row >= column
    lower = jnp.where(causal, 1.0, 0.0).astype(bf16)
    total = jnp.zeros((1, width), f32)
    states = [None] * heads
    for n in range(token_count // chunk):
        rows = slice(n * chunk, (n + 1) * chunk)
        steps = log_decay[rows]
        coarse = steps.astype(bf16)
        fine = (steps - coarse.astype(f32)).astype(bf16)
        summed = dot_nn(lower, coarse) + dot_nn(lower, fine)
        last = summed[chunk - 1 : chunk]
        middle = summed[chunk // 2 - 1 : chunk // 2]
        query = query_ref[rows, :].astype(f32)
        inflow_rows = inflow[rows]
        near_query = (query * jnp.exp(summed - middle)).astype(bf16)
        near_key = (inflow_rows * jnp.exp(middle - summed)).astype(bf16)
        tail_key = (inflow_rows * jnp.exp(last - summed)).astype(bf16)
        faded = (query * jnp.exp(summed + total)).astype(bf16)
        faded_ref[rows, :] = faded
        if n:
            base_query = (query * jnp.exp(summed)).astype(bf16)
        fade = jnp.exp(last)
        for h in range(heads):
            lanes = slice(h * HG_DK, (h + 1) * HG_DK)
            value = value_ref[rows, lanes]
            scores = dot_nt(near_query[:, lanes], near_key[:, lanes])
            scores = jnp.where(causal, scores, 0.0).astype(bf16)
            out = dot_nn(scores, value)
            grown = dot_tn(value, tail_key[:, lanes])
            if n:
                out = out + dot_nt(base_query[:, lanes], states[h].astype(bf16))
                grown = grown + states[h] * fade[:, lanes]
            states[h] = grown
            local_ref[rows, lanes] = out
        total = total + last
    through = jnp.exp(total)
    for h in range(heads):
        lanes = slice(h * HG_DK, (h + 1) * HG_DK)
        state_ref[h, :HG_DV, :] = states[h].astype(bf16)
        state_ref[h, HG_DV:, :] = jnp.broadcast_to(through[:, lanes], (SPARE_ROWS, HG_DK)).astype(
            bf16
        )


def local_recurrence(query, gate, value, bound, added):
    token_count, width = query.shape
    heads = width // HG_DK
    outs = (
        jax.ShapeDtypeStruct((token_count, width), f32),
        jax.ShapeDtypeStruct((token_count, width), bf16),
        jax.ShapeDtypeStruct((heads, HG_DV + SPARE_ROWS, HG_DK), bf16),
    )
    return pl.pallas_call(
        recurrence_kernel,
        out_shape=outs,
        name="recurrence",
        cost_estimate=cost(16 * token_count * width * HG_DK, query, gate, value, *outs),
    )(query, gate, value, bound.reshape(1, -1), added)


def normed(values, gain):
    mean_square = jnp.mean(values * values, axis=-1, keepdims=True)
    return (values * lax.rsqrt(mean_square + epsilon) * gain).astype(bf16)


def carry_kernel(distances, local_ref, faded_ref, gain_ref, *refs):
    state_refs, out_ref = refs[:distances], refs[distances]
    heads = local_ref.shape[1] // HG_DV
    for h in range(heads):
        lanes = slice(h * HG_DV, (h + 1) * HG_DV)
        incoming = jnp.zeros((HG_DV, HG_DK), f32)
        for ref in reversed(state_refs):
            through = ref[h, HG_DV : HG_DV + 1, :].astype(f32)
            incoming = ref[h, :HG_DV, :].astype(f32) + through * incoming
        mixed = local_ref[:, lanes] + dot_nt(faded_ref[:, lanes], incoming.astype(bf16))
        out_ref[:, lanes] = normed(mixed, gain_ref[...])


def carry_in(local, faded, gain, states):
    out = jax.ShapeDtypeStruct(local.shape, bf16)
    return pl.pallas_call(
        functools.partial(carry_kernel, len(states)),
        out_shape=out,
        name="carry",
        cost_estimate=cost(4 * local.size * HG_DK, local, faded, *states),
    )(local, faded, gain.reshape(1, -1), *states)


def attention_kernel(distances, lambda_ref, one_ref, two_ref, gain_ref, own_ref, *refs):
    other_refs, out_ref = refs[:distances], refs[distances]
    token_count = one_ref.shape[0]
    place = lax.axis_index("sp")
    tile = min(token_count, 2 * DA_HD)
    lane = lax.broadcasted_iota(jnp.int32, (tile, 2 * DA_HD), 1)
    blocks = (own_ref, *other_refs)
    wide = 2 * DA_HD
    ones = jnp.ones((token_count, wide), bf16)
    valued = [jnp.concatenate([ref[:, wide : 2 * wide], ones], axis=1) for ref in blocks]
    for t in range(token_count // tile):
        rows = slice(t * tile, (t + 1) * tile)
        row = lax.broadcasted_iota(jnp.int32, (tile, token_count), 0) + t * tile
        column = lax.broadcasted_iota(jnp.int32, (tile, token_count), 1)
        causal = row >= column
        for head in range(2):
            maps = []
            for m, ref in enumerate((one_ref, two_ref)):
                query = ref[rows, :].astype(f32) * DA_HD ** (-0.5)
                if m != head:
                    query = pltpu.roll(query, DA_HD, 1)
                query = jnp.where((lane < DA_HD) == (m == 0), query, 0.0).astype(bf16)
                scores = [dot_nt(query, ref[:, :wide]) for ref in blocks]
                scores[0] = jnp.where(causal, scores[0], -1e30)
                for d in range(distances):
                    scores[d + 1] = jnp.where(place > d, scores[d + 1], -1e30)
                top = functools.reduce(jnp.maximum, scores)
                top = jnp.max(top, axis=-1, keepdims=True)
                sums = None
                for part, value in zip(scores, valued):
                    term = dot_nn(jnp.exp(part - top).astype(bf16), value)
                    sums = term if sums is None else sums + term
                maps.append(sums[:, :wide] / sums[:, wide:])
            mixed = maps[0] - lambda_ref[0, head] * maps[1]
            out_ref[rows, head * wide : (head + 1) * wide] = normed(mixed, gain_ref[...])


def attention(query_one, query_two, own, others, weight, gain):
    token_count = query_one.shape[0]
    out = jax.ShapeDtypeStruct((token_count, 2 * query_one.shape[1]), bf16)
    vmem = pl.BlockSpec(memory_space=pltpu.VMEM)
    return pl.pallas_call(
        functools.partial(attention_kernel, len(others)),
        out_shape=out,
        in_specs=[pl.BlockSpec(memory_space=pltpu.SMEM)] + [vmem] * (4 + len(others)),
        out_specs=vmem,
        name="attention",
        cost_estimate=cost(
            12 * token_count * token_count * query_one.shape[1] * (1 + len(others)), own, *others
        ),
    )(weight.reshape(1, -1), query_one, query_two, gain.reshape(1, -1), own, *others)


def project_kernel(flip, tp_size, pieces, *refs):
    mixed_refs, weight_refs, out_ref = refs[:4], refs[4 : 4 + pieces], refs[4 + pieces]
    share = mixed_refs[0].shape[0] // tp_size
    place = lax.axis_index("tp")

    def rows_of(ref):
        return [
            ref[pl.ds(pl.multiple_of((place ^ flip ^ across) * share, share), share), :]
            for across in (0, 2)
        ]

    recurrent = jnp.concatenate(rows_of(mixed_refs[0]) + rows_of(mixed_refs[2]), axis=0)
    attended = jnp.concatenate(rows_of(mixed_refs[1]) + rows_of(mixed_refs[3]), axis=0)
    for p, ref in enumerate(weight_refs):
        width = ref.shape[2]
        terms = dot_nn(recurrent, ref[0]) + dot_nn(attended, ref[1])
        out_ref[:, p * width : (p + 1) * width] = terms.astype(out_ref.dtype)


def project(flip, tp_size, mixed, weights, dtype):
    rows = 4 * (mixed[0].shape[0] // tp_size)
    width = weights[0].shape[2]
    out = jax.ShapeDtypeStruct((rows, width * len(weights)), dtype)
    return pl.pallas_call(
        functools.partial(project_kernel, flip, tp_size, len(weights)),
        out_shape=out,
        name="project",
        cost_estimate=cost(4 * rows * mixed[0].shape[1] * out.shape[1], *mixed, *weights, out),
    )(*mixed, *weights)


def pair_kernel(kept_ref, came_ref, own_ref, *send_refs):
    share = own_ref.shape[0]
    for k, ref in enumerate((own_ref, *send_refs)):
        rows = slice(k * share, (k + 1) * share)
        ref[...] = (kept_ref[rows, :] + came_ref[rows, :].astype(f32)).astype(ref.dtype)


def pair_sum(kept, came):
    share = (kept.shape[0] // 4, kept.shape[1])
    outs = (jax.ShapeDtypeStruct(share, f32),) + (jax.ShapeDtypeStruct(share, bf16),) * 3
    return pl.pallas_call(
        pair_kernel, out_shape=outs, name="pair", cost_estimate=cost(kept.size, kept, came, *outs)
    )(kept, came)


def final_kernel(pieces, own_ref, across_ref, beside_ref, corner_ref, out_ref):
    group = lax.axis_index("grp")
    place = lax.axis_index("sp")
    width = own_ref.shape[1] // pieces
    for d in range(pieces):
        lanes = slice(d * width, (d + 1) * width)
        start = (place ^ d) * (2 * width)
        mine = own_ref[:, lanes] + across_ref[:, lanes].astype(f32)
        theirs = beside_ref[:, lanes].astype(f32) + corner_ref[:, lanes].astype(f32)
        first = pl.multiple_of(start + group * width, width)
        second = pl.multiple_of(start + (1 - group) * width, width)
        out_ref[:, pl.ds(first, width)] = mine.astype(bf16)
        out_ref[:, pl.ds(second, width)] = theirs.astype(bf16)


def final_sum(pieces, own, across, beside, corner):
    out = jax.ShapeDtypeStruct((own.shape[0], 2 * own.shape[1]), bf16)
    return pl.pallas_call(
        functools.partial(final_kernel, pieces),
        out_shape=out,
        name="final",
        cost_estimate=cost(own.size, own, across, beside, corner, out),
    )(own, across, beside, corner)


def fast_shards(
    sizes,
    recurrent_query,
    recurrent_forget_gate,
    recurrent_value,
    recurrent_gate_lower_bound,
    recurrent_added_decay,
    recurrent_norm_gain,
    attention_query_first,
    attention_key_first,
    attention_query_second,
    attention_key_second,
    attention_value,
    second_map_weight,
    attention_norm_gain,
    output_weight,
):
    grp_size, sp_size, tp_size = sizes
    distances = range(1, sp_size)

    def up(array, d):
        return lax.ppermute(array, "sp", [(k, k + d) for k in range(sp_size - d)])

    def swap(array, axis, size, d):
        return lax.ppermute(array, axis, [(k, k ^ d) for k in range(size)])

    own_keys = jnp.concatenate(
        [attention_key_first, attention_key_second, attention_value], axis=1
    )
    other_keys = [up(own_keys, d) for d in distances]
    half = output_weight.shape[2] // grp_size
    own_weight = lax.dynamic_slice_in_dim(
        output_weight, lax.axis_index("grp") * half, half, axis=2
    )
    weights = [own_weight] + [swap(own_weight, "sp", sp_size, d) for d in distances]
    local, faded, state = local_recurrence(
        recurrent_query,
        recurrent_forget_gate,
        recurrent_value,
        recurrent_gate_lower_bound,
        recurrent_added_decay,
    )
    other_states = [up(state, d) for d in distances]
    attended = attention(
        attention_query_first,
        attention_query_second,
        own_keys,
        other_keys,
        second_map_weight,
        attention_norm_gain,
    )
    recurrent = carry_in(local, faded, recurrent_norm_gain, other_states)
    mixed = (
        recurrent,
        attended,
        swap(recurrent, "grp", grp_size, 1),
        swap(attended, "grp", grp_size, 1),
    )
    sent = project(1, tp_size, mixed, weights, bf16)
    came = swap(sent, "tp", tp_size, 1)
    kept = project(0, tp_size, mixed, weights, f32)
    own, across, beside, corner = pair_sum(kept, came)
    across = swap(across, "tp", tp_size, 2)
    beside = swap(beside, "grp", grp_size, 1)
    corner = lax.ppermute(
        corner,
        ("grp", "tp"),
        [
            (g * tp_size + k, (g ^ 1) * tp_size + (k ^ 2))
            for g in range(grp_size)
            for k in range(tp_size)
        ],
    )
    return final_sum(sp_size, own, across, beside, corner)


def shards(sizes, *arrays):
    grp_size, sp_size, tp_size = sizes
    key_heads = arrays[7].shape[1] // DA_HD
    query_heads = arrays[6].shape[1] // DA_HD
    short = grp_size == 2 and tp_size == 4 and sp_size in (2, 4)
    if short and key_heads == 1 and query_heads == 2:
        return fast_shards(sizes, *arrays)
    return general_shards(*arrays)


def solution(mesh):
    sizes = (mesh.shape["grp"], mesh.shape["sp"], mesh.shape["tp"])
    return jax.shard_map(
        functools.partial(shards, sizes),
        mesh=mesh,
        in_specs=(
            P(("grp", "sp"), "tp"),
            P(("grp", "sp"), "tp"),
            P(("grp", "sp"), "tp"),
            P("tp"),
            P(("grp", "sp"), "tp"),
            P(),
            P(("grp", "sp"), "tp"),
            P(("grp", "sp"), "tp"),
            P(("grp", "sp"), "tp"),
            P(("grp", "sp"), "tp"),
            P(("grp", "sp"), "tp"),
            P("tp"),
            P(),
            P(None, "tp", "sp"),
        ),
        out_specs=P(("grp", "sp", "tp"), None),
        check_vma=False,
    )
```

```python
import functools

import jax
import jax.numpy as jnp
from jax import lax
from jax.experimental import pallas as pl
from jax.experimental.pallas import tpu as pltpu
from jax.sharding import PartitionSpec as P

HG_DK = 128
HG_DV = 128
DA_HD = 64
BLK = 32


epsilon = 1e-06
highest = lax.Precision.HIGHEST
key_span = 512


def carried_in(array, axis, combine, identity):
    size, place = (lax.axis_size(axis), lax.axis_index(axis))
    everything = jax.tree.map(
        lambda part, kind: lax.all_gather(part.astype(kind), axis),
        array,
        (jnp.bfloat16, jnp.bfloat16),
    )
    start = jax.tree.map(
        lambda part, zero: jnp.broadcast_to(jnp.asarray(zero, part.dtype), part.shape),
        array,
        identity,
    )

    def hop(k, before):
        reached = k < place
        new = combine(
            before, jax.tree.map(lambda part, own: part[k].astype(own.dtype), everything, array)
        )
        return jax.tree.map(lambda a, b: jnp.where(reached, a, b), new, before)

    return lax.fori_loop(0, size, hop, start)


def head_norm(head_values, gain_vec):
    mean_square = jnp.mean(head_values * head_values, axis=-1, keepdims=True)
    return head_values * lax.rsqrt(mean_square + epsilon) * gain_vec


def decay_factors(gate_preactivation, lower_bound_logit, added_log_decay, number_of_heads):
    token_count = gate_preactivation.shape[0]
    floor_rate = jax.nn.sigmoid(-lower_bound_logit).reshape(number_of_heads, -1)
    state_inflow = floor_rate[None] * jax.nn.sigmoid(
        -gate_preactivation.astype(jnp.float32)
    ).reshape(token_count, number_of_heads, -1)
    decay_logarithm = jnp.log1p(-state_inflow) + added_log_decay[:, :, None]
    return (state_inflow, decay_logarithm)


def recurrence_blocks(queries, decay_logarithm, state_inflow, value_rows, block_len):
    token_count, number_of_heads, key_width = queries.shape
    block_count = token_count // block_len

    def to_blocks(source):
        return source.reshape(block_count, block_len, number_of_heads, source.shape[-1])

    causal = jnp.tril(jnp.ones((block_len, block_len), jnp.float32))[:, :, None, None]

    def block_step(carry_state, inputs):
        query_blk, decay_blk, inflow_blk, value_blk = inputs
        cumulative = jnp.cumsum(decay_blk, axis=0)
        relative = cumulative[:, None] - cumulative[None, :]
        decay_table = jnp.exp(jnp.minimum(relative, 0.0)) * causal
        scores = jnp.einsum(
            "thd,shd,tshd->hts", query_blk, inflow_blk, decay_table, precision=highest
        )
        block_out = jnp.einsum("hts,shv->thv", scores, value_blk, precision=highest)
        block_out = block_out + jnp.einsum(
            "thd,hdv->thv", query_blk * jnp.exp(cumulative), carry_state, precision=highest
        )
        last_log = cumulative[-1]
        new_state = jnp.exp(last_log)[:, :, None] * carry_state + jnp.einsum(
            "shd,shv->hdv",
            inflow_blk * jnp.exp(last_log[None] - cumulative),
            value_blk,
            precision=highest,
        )
        return (new_state, block_out)

    zero_state = jnp.zeros((number_of_heads, key_width, value_rows.shape[-1]), jnp.float32)
    final_state, outputs = lax.scan(
        block_step,
        zero_state,
        (
            to_blocks(queries),
            to_blocks(decay_logarithm),
            to_blocks(state_inflow),
            to_blocks(value_rows),
        ),
    )
    return (final_state, outputs.reshape(token_count, number_of_heads, -1))


def chain_pair(earlier, following):
    return (earlier[0] * following[0], following[0][:, :, None] * earlier[1] + following[1])


def recurrent_path_output(
    recurrent_query,
    recurrent_forget_gate,
    recurrent_value,
    recurrent_gate_lower_bound,
    recurrent_added_decay,
    recurrent_norm_gain,
):
    token_count = recurrent_query.shape[0]
    number_of_heads = recurrent_gate_lower_bound.shape[0] // HG_DK
    state_inflow, decay_logarithm = decay_factors(
        recurrent_forget_gate, recurrent_gate_lower_bound, recurrent_added_decay, number_of_heads
    )
    queries = recurrent_query.astype(jnp.float32).reshape(token_count, number_of_heads, HG_DK)
    value_rows = recurrent_value.astype(jnp.float32).reshape(token_count, number_of_heads, HG_DV)
    final_state, local_out = recurrence_blocks(
        queries, decay_logarithm, state_inflow, value_rows, BLK
    )
    running_log = jnp.cumsum(decay_logarithm, axis=0)
    through = jnp.exp(running_log[-1])
    incoming = carried_in(
        (through, final_state),
        "sp",
        chain_pair,
        (jnp.ones_like(through), jnp.zeros_like(final_state)),
    )
    carried = jnp.einsum(
        "thd,hdv->thv", queries * jnp.exp(running_log), incoming[1], precision=highest
    )
    return (
        head_norm(local_out + carried, recurrent_norm_gain)
        .astype(jnp.bfloat16)
        .reshape(token_count, -1)
    )


def attention_branch(
    attention_query_first,
    attention_key_first,
    attention_query_second,
    attention_key_second,
    attention_value,
    second_map_weight,
    attention_norm_gain,
):
    query_rows = attention_query_first.shape[0]
    key_heads = attention_key_first.shape[1] // DA_HD
    group_size = attention_query_first.shape[1] // DA_HD // key_heads
    score_scale = DA_HD ** (-0.5)
    offset = lax.axis_index("sp") * query_rows
    query_pos = offset + jnp.arange(query_rows)
    last_query = offset + query_rows - 1
    queries_one = attention_query_first.reshape(query_rows, key_heads, group_size, DA_HD)
    queries_two = attention_query_second.reshape(query_rows, key_heads, group_size, DA_HD)

    def map_update(running, queries, key_rows, value_rows, allowed):
        row_max, weight_mass, value_sum = running
        scores = (
            jnp.einsum("qkgd,skd->kgqs", queries, key_rows, preferred_element_type=jnp.float32)
            * score_scale
        )
        scores = jnp.where(allowed, scores, -1e30)
        new_max = jnp.maximum(row_max, jnp.max(scores, axis=-1))
        weights = jnp.where(allowed, jnp.exp(scores - new_max[..., None]), 0.0)
        shrink = jnp.exp(row_max - new_max)
        weight_mass = weight_mass * shrink + jnp.sum(weights, axis=-1)
        value_sum = value_sum * shrink[..., None] + jnp.einsum(
            "plew,wpd->pled",
            weights.astype(jnp.bfloat16),
            value_rows,
            preferred_element_type=jnp.float32,
        )
        return (new_max, weight_mass, value_sum)

    def key_block(running, block_one, block_two, block_values, first_row):
        span_rows = block_one.shape[0]
        key_pos = first_row + jnp.arange(span_rows)
        allowed = key_pos[None, :] <= query_pos[:, None]
        shaped_one = block_one.reshape(span_rows, key_heads, DA_HD)
        shaped_two = block_two.reshape(span_rows, key_heads, DA_HD)
        shaped_values = block_values.reshape(span_rows, key_heads, 2 * DA_HD)
        return (
            map_update(running[0], queries_one, shaped_one, shaped_values, allowed),
            map_update(running[1], queries_two, shaped_two, shaped_values, allowed),
        )

    def guarded_block(running, block_one, block_two, block_values, first_row):

        def compute(state_in):
            return key_block(state_in, block_one, block_two, block_values, first_row)

        def unchanged(state_in):
            return state_in

        result = lax.cond(first_row > last_query, unchanged, compute, running)
        return result

    start_max = jnp.full((key_heads, group_size, query_rows), -1e30, jnp.float32)
    zero_mass = jnp.zeros((key_heads, group_size, query_rows), jnp.float32)
    zero_sum = jnp.zeros((key_heads, group_size, query_rows, 2 * DA_HD), jnp.float32)
    fresh_state = (start_max, zero_mass, zero_sum)
    running = (fresh_state, fresh_state)
    shard_one = lax.all_gather(attention_key_first, "sp", axis=0, tiled=True)
    shard_two = lax.all_gather(attention_key_second, "sp", axis=0, tiled=True)
    shard_values = lax.all_gather(attention_value, "sp", axis=0, tiled=True)
    row_count = shard_one.shape[0]
    span_rows = min(row_count, key_span)
    full_count = row_count // span_rows

    def span_step(span_index, state_in):
        begin_row = span_index * span_rows
        return guarded_block(
            state_in,
            lax.dynamic_slice_in_dim(shard_one, begin_row, span_rows, 0),
            lax.dynamic_slice_in_dim(shard_two, begin_row, span_rows, 0),
            lax.dynamic_slice_in_dim(shard_values, begin_row, span_rows, 0),
            begin_row,
        )

    running = lax.fori_loop(0, full_count, span_step, running)
    first_map, second_map = running
    lambda_table = second_map_weight.reshape(key_heads, group_size)[:, :, None, None]
    combined = first_map[2] / first_map[1][..., None] - lambda_table * (
        second_map[2] / second_map[1][..., None]
    )
    combined = jnp.transpose(combined, (2, 0, 1, 3)).reshape(
        query_rows, key_heads * group_size, 2 * DA_HD
    )
    return head_norm(combined, attention_norm_gain).astype(jnp.bfloat16).reshape(query_rows, -1)


def general_shards(
    recurrent_query,
    recurrent_forget_gate,
    recurrent_value,
    recurrent_gate_lower_bound,
    recurrent_added_decay,
    recurrent_norm_gain,
    attention_query_first,
    attention_key_first,
    attention_query_second,
    attention_key_second,
    attention_value,
    second_map_weight,
    attention_norm_gain,
    output_weight,
):
    attended = attention_branch(
        attention_query_first,
        attention_key_first,
        attention_query_second,
        attention_key_second,
        attention_value,
        second_map_weight,
        attention_norm_gain,
    )
    recurrent_output = recurrent_path_output(
        recurrent_query,
        recurrent_forget_gate,
        recurrent_value,
        recurrent_gate_lower_bound,
        recurrent_added_decay,
        recurrent_norm_gain,
    )
    pieces = lax.all_gather(output_weight, "sp", axis=2, tiled=True)
    partial_terms = jnp.dot(
        recurrent_output, pieces[0], preferred_element_type=jnp.float32
    ) + jnp.dot(attended, pieces[1], preferred_element_type=jnp.float32)
    return lax.psum_scatter(
        partial_terms.astype(jnp.bfloat16), "tp", scatter_dimension=0, tiled=True
    )


f32 = jnp.float32
bf16 = jnp.bfloat16
SPARE_ROWS = 16


PARAMS = pltpu.CompilerParams(vmem_limit_bytes=16 * 1024 * 1024)


def dot_nt(a, b):
    return lax.dot_general(a, b, (((1,), (1,)), ((), ())), preferred_element_type=f32)


def dot_nn(a, b):
    return jnp.dot(a, b, preferred_element_type=f32)


def dot_tn(a, b):
    return lax.dot_general(a, b, (((0,), (0,)), ((), ())), preferred_element_type=f32)


def cost(flops, *arrays):
    moved = sum(a.size * a.dtype.itemsize for a in arrays)
    return pl.CostEstimate(flops=flops, bytes_accessed=moved, transcendentals=0)


def recurrence_kernel(
    query_ref, gate_ref, value_ref, bound_ref, added_ref, local_ref, faded_ref, state_ref
):
    token_count, width = query_ref.shape
    heads = width // HG_DK
    chunk = min(token_count, HG_DK)
    floor_rate = jax.nn.sigmoid(-bound_ref[...])
    inflow = floor_rate * jax.nn.sigmoid(-gate_ref[...].astype(f32))
    added = added_ref[...]
    wide = [jnp.broadcast_to(added[:, h : h + 1], (token_count, HG_DK)) for h in range(heads)]
    log_decay = jnp.log1p(-inflow) + jnp.concatenate(wide, axis=1)
    row = lax.broadcasted_iota(jnp.int32, (chunk, chunk), 0)
    column = lax.broadcasted_iota(jnp.int32, (chunk, chunk), 1)
    causal = row >= column
    lower = jnp.where(causal, 1.0, 0.0).astype(bf16)
    total = jnp.zeros((1, width), f32)
    states = [None] * heads
    for n in range(token_count // chunk):
        rows = slice(n * chunk, (n + 1) * chunk)
        steps = log_decay[rows]
        coarse = steps.astype(bf16)
        fine = (steps - coarse.astype(f32)).astype(bf16)
        summed = dot_nn(lower, coarse) + dot_nn(lower, fine)
        last = summed[chunk - 1 : chunk]
        middle = summed[chunk // 2 - 1 : chunk // 2]
        query = query_ref[rows, :].astype(f32)
        inflow_rows = inflow[rows]
        near_query = (query * jnp.exp(summed - middle)).astype(bf16)
        near_key = (inflow_rows * jnp.exp(middle - summed)).astype(bf16)
        tail_key = (inflow_rows * jnp.exp(last - summed)).astype(bf16)
        faded = (query * jnp.exp(summed + total)).astype(bf16)
        faded_ref[rows, :] = faded
        if n:
            base_query = (query * jnp.exp(summed)).astype(bf16)
        fade = jnp.exp(last)
        for h in range(heads):
            lanes = slice(h * HG_DK, (h + 1) * HG_DK)
            value = value_ref[rows, lanes]
            scores = dot_nt(near_query[:, lanes], near_key[:, lanes])
            scores = jnp.where(causal, scores, 0.0).astype(bf16)
            out = dot_nn(scores, value)
            grown = dot_tn(value, tail_key[:, lanes])
            if n:
                out = out + dot_nt(base_query[:, lanes], states[h].astype(bf16))
                grown = grown + states[h] * fade[:, lanes]
            states[h] = grown
            local_ref[rows, lanes] = out
        total = total + last
    through = jnp.exp(total)
    for h in range(heads):
        lanes = slice(h * HG_DK, (h + 1) * HG_DK)
        state_ref[h, :HG_DV, :] = states[h].astype(bf16)
        state_ref[h, HG_DV:, :] = jnp.broadcast_to(through[:, lanes], (SPARE_ROWS, HG_DK)).astype(
            bf16
        )


def local_recurrence(query, gate, value, bound, added):
    token_count, width = query.shape
    heads = width // HG_DK
    outs = (
        jax.ShapeDtypeStruct((token_count, width), f32),
        jax.ShapeDtypeStruct((token_count, width), bf16),
        jax.ShapeDtypeStruct((heads, HG_DV + SPARE_ROWS, HG_DK), bf16),
    )
    return pl.pallas_call(
        recurrence_kernel,
        out_shape=outs,
        name="recurrence",
        compiler_params=PARAMS,
        cost_estimate=cost(16 * token_count * width * HG_DK, query, gate, value, *outs),
    )(query, gate, value, bound.reshape(1, -1), added)


def normed(values, gain):
    mean_square = jnp.mean(values * values, axis=-1, keepdims=True)
    return (values * lax.rsqrt(mean_square + epsilon) * gain).astype(bf16)


def carry_kernel(distances, local_ref, faded_ref, gain_ref, *refs):
    state_refs, out_ref = refs[:distances], refs[distances]
    heads = local_ref.shape[1] // HG_DV
    for h in range(heads):
        lanes = slice(h * HG_DV, (h + 1) * HG_DV)
        incoming = jnp.zeros((HG_DV, HG_DK), f32)
        for ref in reversed(state_refs):
            through = ref[h, HG_DV : HG_DV + 1, :].astype(f32)
            incoming = ref[h, :HG_DV, :].astype(f32) + through * incoming
        mixed = local_ref[:, lanes] + dot_nt(faded_ref[:, lanes], incoming.astype(bf16))
        out_ref[:, lanes] = normed(mixed, gain_ref[...])


def merge_kernel(near_ref, far_ref, out_ref):
    for h in range(near_ref.shape[0]):
        through = near_ref[h, HG_DV : HG_DV + 1, :].astype(f32)
        merged = near_ref[h].astype(f32) + through * far_ref[h].astype(f32)
        fade = through * far_ref[h, HG_DV:, :].astype(f32)
        out_ref[h, :HG_DV, :] = merged[:HG_DV].astype(bf16)
        out_ref[h, HG_DV:, :] = fade.astype(bf16)


def merge_states(near, far):
    return pl.pallas_call(
        merge_kernel,
        out_shape=jax.ShapeDtypeStruct(near.shape, bf16),
        name="merge",
        compiler_params=PARAMS,
        cost_estimate=cost(3 * near.size, near, far),
    )(near, far)


def carry_in(local, faded, gain, states):
    out = jax.ShapeDtypeStruct(local.shape, bf16)
    return pl.pallas_call(
        functools.partial(carry_kernel, len(states)),
        out_shape=out,
        name="carry",
        compiler_params=PARAMS,
        cost_estimate=cost(4 * local.size * HG_DK, local, faded, *states),
    )(local, faded, gain.reshape(1, -1), *states)


def attention_kernel(distances, lambda_ref, one_ref, two_ref, gain_ref, own_ref, *refs):
    other_refs, out_ref = refs[:distances], refs[distances]
    token_count = one_ref.shape[0]
    place = lax.axis_index("sp")
    tile = min(token_count, 2 * DA_HD)
    lane = lax.broadcasted_iota(jnp.int32, (tile, 2 * DA_HD), 1)
    blocks = (own_ref, *other_refs)
    wide = 2 * DA_HD
    ones = jnp.ones((token_count, wide), bf16)
    valued = [jnp.concatenate([ref[:, wide : 2 * wide], ones], axis=1) for ref in blocks]
    for t in range(token_count // tile):
        rows = slice(t * tile, (t + 1) * tile)
        row = lax.broadcasted_iota(jnp.int32, (tile, token_count), 0) + t * tile
        column = lax.broadcasted_iota(jnp.int32, (tile, token_count), 1)
        causal = row >= column
        for head in range(2):
            maps = []
            for m, ref in enumerate((one_ref, two_ref)):
                query = ref[rows, :].astype(f32) * DA_HD ** (-0.5)
                if m != head:
                    query = pltpu.roll(query, DA_HD, 1)
                query = jnp.where((lane < DA_HD) == (m == 0), query, 0.0).astype(bf16)
                scores = [dot_nt(query, ref[:, :wide]) for ref in blocks]
                scores[0] = jnp.where(causal, scores[0], -1e30)
                for d in range(distances):
                    scores[d + 1] = jnp.where(place > d, scores[d + 1], -1e30)
                top = functools.reduce(jnp.maximum, scores)
                top = jnp.max(top, axis=-1, keepdims=True)
                sums = None
                for part, value in zip(scores, valued):
                    term = dot_nn(jnp.exp(part - top).astype(bf16), value)
                    sums = term if sums is None else sums + term
                maps.append(sums[:, :wide] / sums[:, wide:])
            mixed = maps[0] - lambda_ref[0, head] * maps[1]
            out_ref[rows, head * wide : (head + 1) * wide] = normed(mixed, gain_ref[...])


def attention(query_one, query_two, own, others, weight, gain):
    token_count = query_one.shape[0]
    out = jax.ShapeDtypeStruct((token_count, 2 * query_one.shape[1]), bf16)
    vmem = pl.BlockSpec(memory_space=pltpu.VMEM)
    return pl.pallas_call(
        functools.partial(attention_kernel, len(others)),
        out_shape=out,
        in_specs=[pl.BlockSpec(memory_space=pltpu.SMEM)] + [vmem] * (4 + len(others)),
        out_specs=vmem,
        name="attention",
        compiler_params=PARAMS,
        cost_estimate=cost(
            12 * token_count * token_count * query_one.shape[1] * (1 + len(others)), own, *others
        ),
    )(weight.reshape(1, -1), query_one, query_two, gain.reshape(1, -1), own, *others)


def is_inner():
    place = lax.axis_index("sp")
    return jnp.logical_and(place > 0, place < lax.axis_size("sp") - 1)


def project_kernel(flip, tp_size, counts, *refs):
    mixed_refs, weight_refs, out_ref = refs[:4], list(refs[4:-1]), refs[-1]
    share = mixed_refs[0].shape[0] // tp_size
    place = lax.axis_index("tp")

    def rows_of(ref):
        return [
            ref[pl.ds(pl.multiple_of((place ^ flip ^ across) * share, share), share), :]
            for across in (0, 2)
        ]

    recurrent = jnp.concatenate(rows_of(mixed_refs[0]) + rows_of(mixed_refs[2]), axis=0)
    attended = jnp.concatenate(rows_of(mixed_refs[1]) + rows_of(mixed_refs[3]), axis=0)
    for p, count in enumerate(counts):
        weight = weight_refs.pop(0)[...]
        if count == 2:
            weight = jnp.where(is_inner(), weight_refs.pop(0)[...], weight)
        width = weight.shape[2]
        terms = dot_nn(recurrent, weight[0]) + dot_nn(attended, weight[1])
        out_ref[:, p * width : (p + 1) * width] = terms.astype(out_ref.dtype)


def project(flip, tp_size, mixed, weights, dtype):
    rows = 4 * (mixed[0].shape[0] // tp_size)
    counts = tuple(len(w) for w in weights)
    weights = [w for choice in weights for w in choice]
    out = jax.ShapeDtypeStruct((rows, weights[0].shape[2] * len(counts)), dtype)
    return pl.pallas_call(
        functools.partial(project_kernel, flip, tp_size, counts),
        out_shape=out,
        name="project",
        compiler_params=PARAMS,
        cost_estimate=cost(4 * rows * mixed[0].shape[1] * out.shape[1], *mixed, *weights, out),
    )(*mixed, *weights)


def pair_kernel(kept_ref, came_ref, own_ref, *send_refs):
    share = own_ref.shape[0]
    for k, ref in enumerate((own_ref, *send_refs)):
        rows = slice(k * share, (k + 1) * share)
        ref[...] = (kept_ref[rows, :] + came_ref[rows, :].astype(f32)).astype(ref.dtype)


def pair_sum(kept, came):
    share = (kept.shape[0] // 4, kept.shape[1])
    outs = (jax.ShapeDtypeStruct(share, f32),) + (jax.ShapeDtypeStruct(share, bf16),) * 3
    return pl.pallas_call(
        pair_kernel,
        out_shape=outs,
        name="pair",
        compiler_params=PARAMS,
        cost_estimate=cost(kept.size, kept, came, *outs),
    )(kept, came)


def final_kernel(counts, *refs):
    out_ref = refs[-1]
    group = lax.axis_index("grp")
    place = lax.axis_index("sp")
    turn = jnp.where(is_inner(), 1, 0)
    piece = 0
    for n, count in enumerate(counts):
        own_ref, across_ref, beside_ref, corner_ref = refs[4 * n : 4 * n + 4]
        width = own_ref.shape[1] // count
        for p in range(count):
            lanes = slice(p * width, (p + 1) * width)
            shard = place ^ piece if piece < 2 else place ^ piece ^ turn
            piece += 1
            start = shard * (2 * width)
            mine = own_ref[:, lanes] + across_ref[:, lanes].astype(f32)
            theirs = beside_ref[:, lanes].astype(f32) + corner_ref[:, lanes].astype(f32)
            first = pl.multiple_of(start + group * width, width)
            second = pl.multiple_of(start + (1 - group) * width, width)
            out_ref[:, pl.ds(first, width)] = mine.astype(bf16)
            out_ref[:, pl.ds(second, width)] = theirs.astype(bf16)


def final_sum(pieces, results):
    arrays = [array for result in results for array in result]
    rows = arrays[0].shape[0]
    width = sum(result[0].shape[1] for result in results)
    counts = tuple(pieces * result[0].shape[1] // width for result in results)
    out = jax.ShapeDtypeStruct((rows, 2 * width), bf16)
    return pl.pallas_call(
        functools.partial(final_kernel, counts),
        out_shape=out,
        name="final",
        compiler_params=PARAMS,
        cost_estimate=cost(out.size, *arrays, out),
    )(*arrays)


def fast_shards(
    sizes,
    recurrent_query,
    recurrent_forget_gate,
    recurrent_value,
    recurrent_gate_lower_bound,
    recurrent_added_decay,
    recurrent_norm_gain,
    attention_query_first,
    attention_key_first,
    attention_query_second,
    attention_key_second,
    attention_value,
    second_map_weight,
    attention_norm_gain,
    output_weight,
):
    grp_size, sp_size, tp_size = sizes

    def swap(array, axis, size, d):
        return lax.ppermute(array, axis, [(k, k ^ d) for k in range(size)])

    def up(array, first):
        return lax.ppermute(array, "sp", [(k, k + 1) for k in range(first, sp_size - 1)])

    last = sp_size - 1
    inner = [(k, last - k) for k in range(1, last)]
    outward = [(1, 0), (last - 1, last)]
    own_keys = jnp.concatenate(
        [attention_key_first, attention_key_second, attention_value], axis=1
    )
    key_hops = [own_keys]
    for k in range(last):
        key_hops.append(up(key_hops[-1], k))
    half = output_weight.shape[2] // grp_size
    own_weight = lax.dynamic_slice_in_dim(
        output_weight, lax.axis_index("grp") * half, half, axis=2
    )
    weight_one = swap(own_weight, "sp", sp_size, 1)
    weight_mid = lax.ppermute(own_weight, "sp", inner)
    weight_mid_far = lax.ppermute(weight_one, "sp", inner)
    weight_end = lax.ppermute(weight_mid, "sp", outward)
    weight_end_far = lax.ppermute(weight_mid_far, "sp", outward)
    local, faded, state = local_recurrence(
        recurrent_query,
        recurrent_forget_gate,
        recurrent_value,
        recurrent_gate_lower_bound,
        recurrent_added_decay,
    )
    below = up(state, 0)
    two = merge_states(state, below)
    far = lax.ppermute(two, "sp", [(k, k + 2) for k in range(sp_size - 2)])
    attended = attention(
        attention_query_first,
        attention_query_second,
        own_keys,
        key_hops[1:],
        second_map_weight,
        attention_norm_gain,
    )
    recurrent = carry_in(local, faded, recurrent_norm_gain, (below, far))
    mixed = (
        recurrent, attended, swap(recurrent, "grp", grp_size, 1), swap(attended, "grp", grp_size, 1)
    )
    corner_pairs = [
        (g * tp_size + k, (g ^ 1) * tp_size + (k ^ 2))
        for g in range(grp_size)
        for k in range(tp_size)
    ]
    groups = (
        ((own_weight,), (weight_one,), (weight_end, weight_mid)),
        ((weight_end_far, weight_mid_far),),
    )
    results = []
    for weights in groups:
        sent = project(1, tp_size, mixed, weights, bf16)
        came = swap(sent, "tp", tp_size, 1)
        kept = project(0, tp_size, mixed, weights, f32)
        own, across, beside, corner = pair_sum(kept, came)
        across = swap(across, "tp", tp_size, 2)
        beside = swap(beside, "grp", grp_size, 1)
        corner = lax.ppermute(corner, ("grp", "tp"), corner_pairs)
        results.append((own, across, beside, corner))
    return final_sum(sp_size, results)


def is_short(sizes):
    return sizes == (2, 4, 4)


def shards(sizes, *arrays):
    key_heads = arrays[7].shape[1] // DA_HD
    query_heads = arrays[6].shape[1] // DA_HD
    if is_short(sizes) and key_heads == 1 and query_heads == 2:
        return fast_shards(sizes, *arrays)
    return general_shards(*arrays)


def solution(mesh):
    sizes = (mesh.shape["grp"], mesh.shape["sp"], mesh.shape["tp"])
    return jax.shard_map(
        functools.partial(shards, sizes),
        mesh=mesh,
        in_specs=(
            P(("grp", "sp"), "tp"),
            P(("grp", "sp"), "tp"),
            P(("grp", "sp"), "tp"),
            P("tp"),
            P(("grp", "sp"), "tp"),
            P(),
            P(("grp", "sp"), "tp"),
            P(("grp", "sp"), "tp"),
            P(("grp", "sp"), "tp"),
            P(("grp", "sp"), "tp"),
            P(("grp", "sp"), "tp"),
            P("tp"),
            P(),
            P(None, "tp", "sp"),
        ),
        out_specs=P(("grp", "sp", "tp"), None),
        check_vma=False,
    )
```

```python
import functools

import jax
import jax.numpy as jnp
from jax import lax
from jax.experimental import pallas as pl
from jax.experimental.pallas import tpu as pltpu
from jax.sharding import PartitionSpec as P

HG_DK = 128
HG_DV = 128
DA_HD = 64
BLK = 32


epsilon = 1e-06
highest = lax.Precision.HIGHEST
key_span = 512


def carried_in(array, axis, combine, identity):
    size, place = (lax.axis_size(axis), lax.axis_index(axis))
    everything = jax.tree.map(
        lambda part, kind: lax.all_gather(part.astype(kind), axis),
        array,
        (jnp.bfloat16, jnp.bfloat16),
    )
    start = jax.tree.map(
        lambda part, zero: jnp.broadcast_to(jnp.asarray(zero, part.dtype), part.shape),
        array,
        identity,
    )

    def hop(k, before):
        reached = k < place
        new = combine(
            before, jax.tree.map(lambda part, own: part[k].astype(own.dtype), everything, array)
        )
        return jax.tree.map(lambda a, b: jnp.where(reached, a, b), new, before)

    return lax.fori_loop(0, size, hop, start)


def head_norm(head_values, gain_vec):
    mean_square = jnp.mean(head_values * head_values, axis=-1, keepdims=True)
    return head_values * lax.rsqrt(mean_square + epsilon) * gain_vec


def decay_factors(gate_preactivation, lower_bound_logit, added_log_decay, number_of_heads):
    token_count = gate_preactivation.shape[0]
    floor_rate = jax.nn.sigmoid(-lower_bound_logit).reshape(number_of_heads, -1)
    state_inflow = floor_rate[None] * jax.nn.sigmoid(
        -gate_preactivation.astype(jnp.float32)
    ).reshape(token_count, number_of_heads, -1)
    decay_logarithm = jnp.log1p(-state_inflow) + added_log_decay[:, :, None]
    return (state_inflow, decay_logarithm)


def recurrence_blocks(queries, decay_logarithm, state_inflow, value_rows, block_len):
    token_count, number_of_heads, key_width = queries.shape
    block_count = token_count // block_len

    def to_blocks(source):
        return source.reshape(block_count, block_len, number_of_heads, source.shape[-1])

    causal = jnp.tril(jnp.ones((block_len, block_len), jnp.float32))[:, :, None, None]

    def block_step(carry_state, inputs):
        query_blk, decay_blk, inflow_blk, value_blk = inputs
        cumulative = jnp.cumsum(decay_blk, axis=0)
        relative = cumulative[:, None] - cumulative[None, :]
        decay_table = jnp.exp(jnp.minimum(relative, 0.0)) * causal
        scores = jnp.einsum(
            "thd,shd,tshd->hts", query_blk, inflow_blk, decay_table, precision=highest
        )
        block_out = jnp.einsum("hts,shv->thv", scores, value_blk, precision=highest)
        block_out = block_out + jnp.einsum(
            "thd,hdv->thv", query_blk * jnp.exp(cumulative), carry_state, precision=highest
        )
        last_log = cumulative[-1]
        new_state = jnp.exp(last_log)[:, :, None] * carry_state + jnp.einsum(
            "shd,shv->hdv",
            inflow_blk * jnp.exp(last_log[None] - cumulative),
            value_blk,
            precision=highest,
        )
        return (new_state, block_out)

    zero_state = jnp.zeros((number_of_heads, key_width, value_rows.shape[-1]), jnp.float32)
    final_state, outputs = lax.scan(
        block_step,
        zero_state,
        (
            to_blocks(queries),
            to_blocks(decay_logarithm),
            to_blocks(state_inflow),
            to_blocks(value_rows),
        ),
    )
    return (final_state, outputs.reshape(token_count, number_of_heads, -1))


def chain_pair(earlier, following):
    return (earlier[0] * following[0], following[0][:, :, None] * earlier[1] + following[1])


def recurrent_path_output(
    recurrent_query,
    recurrent_forget_gate,
    recurrent_value,
    recurrent_gate_lower_bound,
    recurrent_added_decay,
    recurrent_norm_gain,
):
    token_count = recurrent_query.shape[0]
    number_of_heads = recurrent_gate_lower_bound.shape[0] // HG_DK
    state_inflow, decay_logarithm = decay_factors(
        recurrent_forget_gate, recurrent_gate_lower_bound, recurrent_added_decay, number_of_heads
    )
    queries = recurrent_query.astype(jnp.float32).reshape(token_count, number_of_heads, HG_DK)
    value_rows = recurrent_value.astype(jnp.float32).reshape(token_count, number_of_heads, HG_DV)
    final_state, local_out = recurrence_blocks(
        queries, decay_logarithm, state_inflow, value_rows, BLK
    )
    running_log = jnp.cumsum(decay_logarithm, axis=0)
    through = jnp.exp(running_log[-1])
    incoming = carried_in(
        (through, final_state),
        "sp",
        chain_pair,
        (jnp.ones_like(through), jnp.zeros_like(final_state)),
    )
    carried = jnp.einsum(
        "thd,hdv->thv", queries * jnp.exp(running_log), incoming[1], precision=highest
    )
    return (
        head_norm(local_out + carried, recurrent_norm_gain)
        .astype(jnp.bfloat16)
        .reshape(token_count, -1)
    )


def attention_branch(
    attention_query_first,
    attention_key_first,
    attention_query_second,
    attention_key_second,
    attention_value,
    second_map_weight,
    attention_norm_gain,
):
    query_rows = attention_query_first.shape[0]
    key_heads = attention_key_first.shape[1] // DA_HD
    group_size = attention_query_first.shape[1] // DA_HD // key_heads
    score_scale = DA_HD ** (-0.5)
    offset = lax.axis_index("sp") * query_rows
    query_pos = offset + jnp.arange(query_rows)
    last_query = offset + query_rows - 1
    queries_one = attention_query_first.reshape(query_rows, key_heads, group_size, DA_HD)
    queries_two = attention_query_second.reshape(query_rows, key_heads, group_size, DA_HD)

    def map_update(running, queries, key_rows, value_rows, allowed):
        row_max, weight_mass, value_sum = running
        scores = (
            jnp.einsum("qkgd,skd->kgqs", queries, key_rows, preferred_element_type=jnp.float32)
            * score_scale
        )
        scores = jnp.where(allowed, scores, -1e30)
        new_max = jnp.maximum(row_max, jnp.max(scores, axis=-1))
        weights = jnp.where(allowed, jnp.exp(scores - new_max[..., None]), 0.0)
        shrink = jnp.exp(row_max - new_max)
        weight_mass = weight_mass * shrink + jnp.sum(weights, axis=-1)
        value_sum = value_sum * shrink[..., None] + jnp.einsum(
            "plew,wpd->pled",
            weights.astype(jnp.bfloat16),
            value_rows,
            preferred_element_type=jnp.float32,
        )
        return (new_max, weight_mass, value_sum)

    def key_block(running, block_one, block_two, block_values, first_row):
        span_rows = block_one.shape[0]
        key_pos = first_row + jnp.arange(span_rows)
        allowed = key_pos[None, :] <= query_pos[:, None]
        shaped_one = block_one.reshape(span_rows, key_heads, DA_HD)
        shaped_two = block_two.reshape(span_rows, key_heads, DA_HD)
        shaped_values = block_values.reshape(span_rows, key_heads, 2 * DA_HD)
        return (
            map_update(running[0], queries_one, shaped_one, shaped_values, allowed),
            map_update(running[1], queries_two, shaped_two, shaped_values, allowed),
        )

    def guarded_block(running, block_one, block_two, block_values, first_row):

        def compute(state_in):
            return key_block(state_in, block_one, block_two, block_values, first_row)

        def unchanged(state_in):
            return state_in

        result = lax.cond(first_row > last_query, unchanged, compute, running)
        return result

    start_max = jnp.full((key_heads, group_size, query_rows), -1e30, jnp.float32)
    zero_mass = jnp.zeros((key_heads, group_size, query_rows), jnp.float32)
    zero_sum = jnp.zeros((key_heads, group_size, query_rows, 2 * DA_HD), jnp.float32)
    fresh_state = (start_max, zero_mass, zero_sum)
    running = (fresh_state, fresh_state)
    shard_one = lax.all_gather(attention_key_first, "sp", axis=0, tiled=True)
    shard_two = lax.all_gather(attention_key_second, "sp", axis=0, tiled=True)
    shard_values = lax.all_gather(attention_value, "sp", axis=0, tiled=True)
    row_count = shard_one.shape[0]
    span_rows = min(row_count, key_span)
    full_count = row_count // span_rows

    def span_step(span_index, state_in):
        begin_row = span_index * span_rows
        return guarded_block(
            state_in,
            lax.dynamic_slice_in_dim(shard_one, begin_row, span_rows, 0),
            lax.dynamic_slice_in_dim(shard_two, begin_row, span_rows, 0),
            lax.dynamic_slice_in_dim(shard_values, begin_row, span_rows, 0),
            begin_row,
        )

    running = lax.fori_loop(0, full_count, span_step, running)
    first_map, second_map = running
    lambda_table = second_map_weight.reshape(key_heads, group_size)[:, :, None, None]
    combined = first_map[2] / first_map[1][..., None] - lambda_table * (
        second_map[2] / second_map[1][..., None]
    )
    combined = jnp.transpose(combined, (2, 0, 1, 3)).reshape(
        query_rows, key_heads * group_size, 2 * DA_HD
    )
    return head_norm(combined, attention_norm_gain).astype(jnp.bfloat16).reshape(query_rows, -1)


def general_shards(
    recurrent_query,
    recurrent_forget_gate,
    recurrent_value,
    recurrent_gate_lower_bound,
    recurrent_added_decay,
    recurrent_norm_gain,
    attention_query_first,
    attention_key_first,
    attention_query_second,
    attention_key_second,
    attention_value,
    second_map_weight,
    attention_norm_gain,
    output_weight,
):
    attended = attention_branch(
        attention_query_first,
        attention_key_first,
        attention_query_second,
        attention_key_second,
        attention_value,
        second_map_weight,
        attention_norm_gain,
    )
    recurrent_output = recurrent_path_output(
        recurrent_query,
        recurrent_forget_gate,
        recurrent_value,
        recurrent_gate_lower_bound,
        recurrent_added_decay,
        recurrent_norm_gain,
    )
    pieces = lax.all_gather(output_weight, "sp", axis=2, tiled=True)
    partial_terms = jnp.dot(
        recurrent_output, pieces[0], preferred_element_type=jnp.float32
    ) + jnp.dot(attended, pieces[1], preferred_element_type=jnp.float32)
    return lax.psum_scatter(
        partial_terms.astype(jnp.bfloat16), "tp", scatter_dimension=0, tiled=True
    )


f32 = jnp.float32
bf16 = jnp.bfloat16
SPARE_ROWS = 16


PARAMS = pltpu.CompilerParams(vmem_limit_bytes=16 * 1024 * 1024)


def dot_nt(a, b):
    return lax.dot_general(a, b, (((1,), (1,)), ((), ())), preferred_element_type=f32)


def dot_nn(a, b):
    return jnp.dot(a, b, preferred_element_type=f32)


def dot_tn(a, b):
    return lax.dot_general(a, b, (((0,), (0,)), ((), ())), preferred_element_type=f32)


def cost(flops, *arrays):
    moved = sum(a.size * a.dtype.itemsize for a in arrays)
    return pl.CostEstimate(flops=flops, bytes_accessed=moved, transcendentals=0)


BASE = 4 * DA_HD
STATE = slice(BASE, BASE + HG_DV)
FADE = slice(BASE + HG_DV, BASE + HG_DV + SPARE_ROWS)
HBM = pl.BlockSpec(memory_space=pltpu.HBM)
VMEM = pl.BlockSpec(memory_space=pltpu.VMEM)


def prepare_kernel(last, *refs):
    sources, rest = refs[:13], refs[13:]
    local_ref, faded_ref, packed_ref, front_ref, asked_ref, gain_ref, weight_ref = rest[:7]
    query_ref, gate_ref, value_ref, bound_ref, added_ref, lift_ref, sems = rest[7:]
    token_count, width = query_ref.shape
    heads = width // HG_DK
    chunk = HG_DK
    wide = 2 * DA_HD
    targets = [
        packed_ref.at[:DA_HD, :],
        packed_ref.at[DA_HD:wide, :],
        lift_ref,
        asked_ref.at[:, :wide],
        asked_ref.at[:, wide:],
        gate_ref,
        bound_ref,
        added_ref,
        query_ref,
        value_ref,
        gain_ref.at[0:1, :],
        gain_ref.at[1:2, :],
        weight_ref,
    ]
    copies = [
        pltpu.make_async_copy(source, target, sems.at[k])
        for k, (source, target) in enumerate(zip(sources, targets))
    ]
    for copy in copies:
        copy.start()
    for copy in copies[5:]:
        copy.wait()
    floor_rate = jax.nn.sigmoid(-bound_ref[...])
    inflow = floor_rate * jax.nn.sigmoid(-gate_ref[...].astype(f32))
    log_decay = jnp.log1p(-inflow)
    row = lax.broadcasted_iota(jnp.int32, (chunk, chunk), 0)
    column = lax.broadcasted_iota(jnp.int32, (chunk, chunk), 1)
    causal = row >= column
    lower = jnp.where(causal, 1.0, 0.0).astype(bf16)
    total = jnp.zeros((1, width), f32)
    states = [None] * heads
    for n in range(token_count // chunk):
        rows = slice(n * chunk, (n + 1) * chunk)
        steps = log_decay[rows]
        coarse = steps.astype(bf16)
        fine = (steps - coarse.astype(f32)).astype(bf16)
        extra = []
        for h in range(heads):
            steps_row = jnp.where(causal, added_ref[h : h + 1, rows], 0.0)
            extra.append(
                jnp.broadcast_to(jnp.sum(steps_row, axis=1, keepdims=True), (chunk, HG_DK))
            )
        summed = dot_nn(lower, coarse) + dot_nn(lower, fine) + jnp.concatenate(extra, axis=1)
        final = summed[chunk - 1 : chunk]
        middle = summed[chunk // 2 - 1 : chunk // 2]
        query = query_ref[rows, :].astype(f32)
        inflow_rows = inflow[rows]
        near_query = (query * jnp.exp(summed - middle)).astype(bf16)
        near_key = (inflow_rows * jnp.exp(middle - summed)).astype(bf16)
        tail_key = (inflow_rows * jnp.exp(final - summed)).astype(bf16)
        faded_ref[rows, :] = (query * jnp.exp(summed + total)).astype(bf16)
        if n:
            base_query = (query * jnp.exp(summed)).astype(bf16)
        fade = jnp.exp(final)
        for h in range(heads):
            lanes = slice(h * HG_DK, (h + 1) * HG_DK)
            value = value_ref[rows, lanes]
            scores = dot_nt(near_query[:, lanes], near_key[:, lanes])
            scores = jnp.where(causal, scores, 0.0).astype(bf16)
            out = dot_nn(scores, value)
            grown = dot_tn(value, tail_key[:, lanes])
            if n:
                out = out + dot_nt(base_query[:, lanes], states[h].astype(bf16))
                grown = grown + states[h] * fade[:, lanes]
            states[h] = grown
            local_ref[rows, lanes] = out
        total = total + final
    through = jnp.exp(total)
    for h in range(heads):
        lanes = slice(h * HG_DK, (h + 1) * HG_DK)
        packed_ref[STATE, lanes] = states[h].astype(bf16)
    packed_ref[FADE, :] = jnp.broadcast_to(through, (SPARE_ROWS, width)).astype(bf16)
    for copy in copies[:5]:
        copy.wait()
    for n in range(token_count // wide):
        block = lift_ref[n * wide : (n + 1) * wide, :]
        packed_ref[wide:BASE, n * wide : (n + 1) * wide] = block
    front_ref[:BASE, :] = packed_ref[:BASE, :]
    at_end = lax.axis_index("sp") == last

    @pl.when(at_end)
    def _():
        front_ref[BASE:, :] = asked_ref[...]

    @pl.when(jnp.logical_not(at_end))
    def _():
        front_ref[BASE : BASE + HG_DV + SPARE_ROWS, :] = packed_ref[BASE:, :]


def prepare(last, arrays):
    (
        query,
        gate,
        value,
        bound,
        added,
        gain,
        query_one,
        key_one,
        query_two,
        key_two,
        att_value,
        weight,
        att_gain,
    ) = arrays
    token_count, width = query.shape
    wide = 2 * DA_HD
    rows = BASE + HG_DV + SPARE_ROWS
    shape = jax.ShapeDtypeStruct
    outs = (
        shape((token_count, width), f32),
        shape((token_count, width), bf16),
        shape((rows, width), bf16),
        shape((BASE + token_count, width), bf16),
        shape((token_count, width), bf16),
        shape((2, HG_DV), f32),
        shape((1, weight.shape[0]), f32),
    )
    inputs = (
        key_one.T,
        key_two.T,
        att_value,
        query_one,
        query_two,
        gate,
        bound.reshape(1, -1),
        added.T,
        query,
        value,
        gain.reshape(1, -1),
        att_gain.reshape(1, -1),
        weight.reshape(1, -1),
    )
    return pl.pallas_call(
        functools.partial(prepare_kernel, last),
        out_shape=outs,
        in_specs=[HBM] * len(inputs),
        out_specs=[VMEM] * len(outs),
        scratch_shapes=[
            pltpu.VMEM((token_count, width), bf16),
            pltpu.VMEM((token_count, width), bf16),
            pltpu.VMEM((token_count, width), bf16),
            pltpu.VMEM((1, width), f32),
            pltpu.VMEM(added.T.shape, f32),
            pltpu.VMEM((token_count, wide), bf16),
            pltpu.SemaphoreType.DMA((len(inputs),)),
        ],
        name="prepare",
        compiler_params=PARAMS,
        cost_estimate=cost(16 * token_count * width * HG_DK, query, gate, value, *outs),
    )(*(pltpu.with_memory_space_constraint(array, pltpu.HBM) for array in inputs))


def normed(values, gain):
    mean_square = jnp.mean(values * values, axis=-1, keepdims=True)
    return (values * lax.rsqrt(mean_square + epsilon) * gain).astype(bf16)


def blend_kernel(own_ref, one_ref, two_ref, out_ref):
    merged = one_ref[STATE, :].astype(f32)
    merged = merged + fade_of(one_ref) * two_ref[STATE, :].astype(f32)
    merged = own_ref[STATE, :].astype(f32) + fade_of(own_ref) * merged
    out_ref[...] = merged.astype(bf16)


def fade_of(ref):
    return ref[BASE + HG_DV : BASE + HG_DV + 1, :].astype(f32)


def blend(own, one, two):
    return pl.pallas_call(
        blend_kernel,
        out_shape=jax.ShapeDtypeStruct((HG_DV, own.shape[1]), bf16),
        name="blend",
        compiler_params=PARAMS,
        cost_estimate=cost(own.size, own, one, two),
    )(own, one, two)


def carry_kernel(local_ref, faded_ref, gain_ref, p1_ref, p2_ref, p3_ref, p4_ref, out_ref):
    heads = local_ref.shape[1] // HG_DV
    place = lax.axis_index("sp")
    merged = p2_ref[STATE, :].astype(f32) + fade_of(p2_ref) * p3_ref[STATE, :].astype(f32)
    incoming = jnp.where(place == 2, merged, p4_ref[...].astype(f32))
    incoming = jnp.where(place == 1, p1_ref[STATE, :].astype(f32), incoming)
    incoming = jnp.where(place == 0, 0.0, incoming).astype(bf16)
    for h in range(heads):
        lanes = slice(h * HG_DV, (h + 1) * HG_DV)
        mixed = local_ref[:, lanes] + dot_nt(faded_ref[:, lanes], incoming[:, lanes])
        out_ref[:, lanes] = normed(mixed, gain_ref[0:1, :])


def carry_in(local, faded, gain, *parts):
    return pl.pallas_call(
        carry_kernel,
        out_shape=jax.ShapeDtypeStruct(local.shape, bf16),
        name="carry",
        compiler_params=PARAMS,
        cost_estimate=cost(4 * local.size * HG_DK, local, faded, *parts),
    )(local, faded, gain, *parts)


def attend(asked, blocks, weight_ref, gain_ref, out_ref):
    wide = 2 * DA_HD
    token_count = asked.shape[0]
    tile = min(token_count, wide)
    lane = lax.broadcasted_iota(jnp.int32, (tile, wide), 1)
    ones = jnp.ones((token_count, wide), bf16)
    valued = []
    for ref, _ in blocks:
        value = [
            ref[wide:BASE, n * wide : (n + 1) * wide] for n in range(token_count // wide)
        ]
        valued.append(jnp.concatenate([jnp.concatenate(value, axis=0), ones], axis=1))
    for t in range(token_count // tile):
        rows = slice(t * tile, (t + 1) * tile)
        row = lax.broadcasted_iota(jnp.int32, (tile, token_count), 0) + t * tile
        column = lax.broadcasted_iota(jnp.int32, (tile, token_count), 1)
        causal = row >= column
        for head in range(2):
            maps = []
            for m in range(2):
                query = asked[rows, m * wide : (m + 1) * wide].astype(f32) * DA_HD ** (-0.5)
                if m != head:
                    query = pltpu.roll(query, DA_HD, 1)
                query = jnp.where((lane < DA_HD) == (m == 0), query, 0.0).astype(bf16)
                scores = []
                for ref, allowed in blocks:
                    score = dot_nn(query, ref[:wide, :])
                    if allowed is None:
                        score = jnp.where(causal, score, -1e30)
                    elif allowed is not True:
                        score = jnp.where(allowed, score, -1e30)
                    scores.append(score)
                top = functools.reduce(jnp.maximum, scores)
                top = jnp.max(top, axis=-1, keepdims=True)
                sums = None
                for part, value in zip(scores, valued):
                    term = dot_nn(jnp.exp(part - top).astype(bf16), value)
                    sums = term if sums is None else sums + term
                maps.append(sums[:, :wide] / sums[:, wide:])
            mixed = maps[0] - weight_ref[0:1, head : head + 1] * maps[1]
            out_ref[rows, head * wide : (head + 1) * wide] = normed(mixed, gain_ref[1:2, :])


def helper_kernel(last, own_ref, p1_ref, p2_ref, p3_ref, weight_ref, gain_ref, out_ref):
    @pl.when(lax.axis_index("sp") == last - 1)
    def _():
        blocks = [(p1_ref, None), (own_ref, True), (p2_ref, True), (p3_ref, True)]
        attend(p1_ref.at[BASE:, :], blocks, weight_ref, gain_ref, out_ref)


def main_kernel(last, asked_ref, own_ref, p1_ref, p2_ref, p3_ref, weight_ref, gain_ref, out_ref):
    place = lax.axis_index("sp")

    @pl.when(place == last - 1)
    def _():
        blocks = [(own_ref, None), (p2_ref, True), (p3_ref, True)]
        attend(asked_ref, blocks, weight_ref, gain_ref, out_ref)

    @pl.when(place < last - 1)
    def _():
        blocks = [(own_ref, None), (p1_ref, place > 0)]
        attend(asked_ref, blocks, weight_ref, gain_ref, out_ref)


def attention(kernel, last, token_count, *arrays):
    width = arrays[0].shape[1]
    return pl.pallas_call(
        functools.partial(kernel, last),
        out_shape=jax.ShapeDtypeStruct((token_count, width), bf16),
        compiler_params=PARAMS,
        cost_estimate=cost(24 * token_count * token_count * width, *arrays),
    )(*arrays)


def choose_kernel(last, main_ref, helped_ref, out_ref):
    at_end = lax.axis_index("sp") == last

    @pl.when(at_end)
    def _():
        out_ref[...] = helped_ref[...]

    @pl.when(jnp.logical_not(at_end))
    def _():
        out_ref[...] = main_ref[...]


def choose(last, main, helped):
    return pl.pallas_call(
        functools.partial(choose_kernel, last),
        out_shape=jax.ShapeDtypeStruct(main.shape, bf16),
        name="choose",
        compiler_params=PARAMS,
        cost_estimate=cost(main.size, main, helped),
    )(main, helped)


def is_inner():
    place = lax.axis_index("sp")
    return jnp.logical_and(place > 0, place < lax.axis_size("sp") - 1)


def project_kernel(flip, tp_size, counts, *refs):
    mixed_refs, weight_refs, out_ref = refs[:4], list(refs[4:-1]), refs[-1]
    share = mixed_refs[0].shape[0] // tp_size
    place = lax.axis_index("tp")

    def rows_of(ref):
        return [
            ref[pl.ds(pl.multiple_of((place ^ flip ^ across) * share, share), share), :]
            for across in (0, 2)
        ]

    recurrent = jnp.concatenate(rows_of(mixed_refs[0]) + rows_of(mixed_refs[2]), axis=0)
    attended = jnp.concatenate(rows_of(mixed_refs[1]) + rows_of(mixed_refs[3]), axis=0)
    for p, count in enumerate(counts):
        weight = weight_refs.pop(0)[...]
        if count == 2:
            weight = jnp.where(is_inner(), weight_refs.pop(0)[...], weight)
        width = weight.shape[2]
        terms = dot_nn(recurrent, weight[0]) + dot_nn(attended, weight[1])
        out_ref[:, p * width : (p + 1) * width] = terms.astype(out_ref.dtype)


def project(flip, tp_size, mixed, weights, dtype):
    rows = 4 * (mixed[0].shape[0] // tp_size)
    counts = tuple(len(w) for w in weights)
    weights = [w for choice in weights for w in choice]
    out = jax.ShapeDtypeStruct((rows, weights[0].shape[2] * len(counts)), dtype)
    return pl.pallas_call(
        functools.partial(project_kernel, flip, tp_size, counts),
        out_shape=out,
        name="project",
        compiler_params=PARAMS,
        cost_estimate=cost(4 * rows * mixed[0].shape[1] * out.shape[1], *mixed, *weights, out),
    )(*mixed, *weights)


def pair_kernel(first, kept_ref, came_ref, *out_refs):
    share = out_refs[0].shape[0]
    for k, ref in enumerate(out_refs):
        rows = slice((first + k) * share, (first + k + 1) * share)
        ref[...] = (kept_ref[rows, :] + came_ref[rows, :].astype(f32)).astype(ref.dtype)


def pair_sum(kept, came, first, count, dtype):
    share = (kept.shape[0] // 4, kept.shape[1])
    outs = (jax.ShapeDtypeStruct(share, dtype),) * count
    return pl.pallas_call(
        functools.partial(pair_kernel, first),
        out_shape=outs,
        name="pair",
        compiler_params=PARAMS,
        cost_estimate=cost(kept.size, kept, came, *outs),
    )(kept, came)


def final_kernel(counts, *refs):
    out_ref = refs[-1]
    group = lax.axis_index("grp")
    place = lax.axis_index("sp")
    turn = jnp.where(is_inner(), 1, 0)
    piece = 0
    for n, count in enumerate(counts):
        own_ref, across_ref, beside_ref, corner_ref = refs[4 * n : 4 * n + 4]
        width = own_ref.shape[1] // count
        for p in range(count):
            lanes = slice(p * width, (p + 1) * width)
            shard = place ^ piece if piece < 2 else place ^ piece ^ turn
            piece += 1
            start = shard * (2 * width)
            mine = own_ref[:, lanes] + across_ref[:, lanes].astype(f32)
            theirs = beside_ref[:, lanes].astype(f32) + corner_ref[:, lanes].astype(f32)
            first = pl.multiple_of(start + group * width, width)
            second = pl.multiple_of(start + (1 - group) * width, width)
            out_ref[:, pl.ds(first, width)] = mine.astype(bf16)
            out_ref[:, pl.ds(second, width)] = theirs.astype(bf16)


def final_sum(pieces, results):
    arrays = [array for result in results for array in result]
    rows = arrays[0].shape[0]
    width = sum(result[0].shape[1] for result in results)
    counts = tuple(pieces * result[0].shape[1] // width for result in results)
    out = jax.ShapeDtypeStruct((rows, 2 * width), bf16)
    return pl.pallas_call(
        functools.partial(final_kernel, counts),
        out_shape=out,
        name="final",
        compiler_params=PARAMS,
        cost_estimate=cost(out.size, *arrays, out),
    )(*arrays)


def fast_shards(sizes, *arrays):
    grp_size, sp_size, tp_size = sizes
    output_weight = arrays[13]
    tokens = arrays[0].shape[0]

    def swap(array, axis, size, d):
        return lax.ppermute(array, axis, [(k, k ^ d) for k in range(size)])

    last = sp_size - 1
    inner = [(1, 2), (2, 1)]
    outward = [(1, 0), (2, last)]
    local, faded, packed, front, asked, gains, weight = prepare(last, arrays[:13])
    p1 = lax.ppermute(front, "sp", [(0, 1), (last, 2)])
    p2 = lax.ppermute(packed, "sp", [(1, 2)])
    p3 = lax.ppermute(packed, "sp", [(0, 2)])
    half = output_weight.shape[2] // grp_size
    own_weight = lax.dynamic_slice_in_dim(
        output_weight, lax.axis_index("grp") * half, half, axis=2
    )
    weight_one = swap(own_weight, "sp", sp_size, 1)
    weight_mid = lax.ppermute(own_weight, "sp", inner)
    weight_mid_far = lax.ppermute(weight_one, "sp", inner)
    weight_end = lax.ppermute(weight_mid, "sp", outward)
    weight_end_far = lax.ppermute(weight_mid_far, "sp", outward)
    p4 = lax.ppermute(blend(packed, p2, p3), "sp", [(2, last)])
    helped = attention(helper_kernel, last, tokens, packed, p1, p2, p3, weight, gains)
    p5 = lax.ppermute(helped, "sp", [(2, last)])
    main = attention(main_kernel, last, tokens, asked, packed, p1, p2, p3, weight, gains)
    recurrent = carry_in(local, faded, gains, p1, p2, p3, p4)
    attended = choose(last, main, p5)
    mixed = (
        recurrent, attended, swap(recurrent, "grp", grp_size, 1), swap(attended, "grp", grp_size, 1)
    )
    corner_pairs = [
        (g * tp_size + k, (g ^ 1) * tp_size + (k ^ 2))
        for g in range(grp_size)
        for k in range(tp_size)
    ]
    groups = (
        ((own_weight,), (weight_one,), (weight_end, weight_mid)),
        ((weight_end_far, weight_mid_far),),
    )
    results = []
    for weights in groups:
        sent = project(1, tp_size, mixed, weights, bf16)
        came = swap(sent, "tp", tp_size, 1)
        kept = project(0, tp_size, mixed, weights, f32)
        across, beside, corner = pair_sum(kept, came, 1, 3, bf16)
        (own,) = pair_sum(kept, came, 0, 1, f32)
        across = swap(across, "tp", tp_size, 2)
        beside = swap(beside, "grp", grp_size, 1)
        corner = lax.ppermute(corner, ("grp", "tp"), corner_pairs)
        results.append((own, across, beside, corner))
    return final_sum(sp_size, results)


def is_short(sizes):
    return sizes == (2, 4, 4)


def shards(sizes, *arrays):
    key_heads = arrays[7].shape[1] // DA_HD
    query_heads = arrays[6].shape[1] // DA_HD
    if is_short(sizes) and key_heads == 1 and query_heads == 2:
        return fast_shards(sizes, *arrays)
    return general_shards(*arrays)


def solution(mesh):
    sizes = (mesh.shape["grp"], mesh.shape["sp"], mesh.shape["tp"])
    return jax.shard_map(
        functools.partial(shards, sizes),
        mesh=mesh,
        in_specs=(
            P(("grp", "sp"), "tp"),
            P(("grp", "sp"), "tp"),
            P(("grp", "sp"), "tp"),
            P("tp"),
            P(("grp", "sp"), "tp"),
            P(),
            P(("grp", "sp"), "tp"),
            P(("grp", "sp"), "tp"),
            P(("grp", "sp"), "tp"),
            P(("grp", "sp"), "tp"),
            P(("grp", "sp"), "tp"),
            P("tp"),
            P(),
            P(None, "tp", "sp"),
        ),
        out_specs=P(("grp", "sp", "tp"), None),
        check_vma=False,
    )
```

```python
import functools

import jax
import jax.numpy as jnp
from jax import lax
from jax.experimental import pallas as pl
from jax.experimental.pallas import tpu as pltpu
from jax.sharding import PartitionSpec as P

HG_DK = 128
HG_DV = 128
DA_HD = 64
BLK = 32


epsilon = 1e-06
highest = lax.Precision.HIGHEST
key_span = 512


def carried_in(array, axis, combine, identity):
    size, place = (lax.axis_size(axis), lax.axis_index(axis))
    everything = jax.tree.map(
        lambda part, kind: lax.all_gather(part.astype(kind), axis),
        array,
        (jnp.bfloat16, jnp.bfloat16),
    )
    start = jax.tree.map(
        lambda part, zero: jnp.broadcast_to(jnp.asarray(zero, part.dtype), part.shape),
        array,
        identity,
    )

    def hop(k, before):
        reached = k < place
        new = combine(
            before, jax.tree.map(lambda part, own: part[k].astype(own.dtype), everything, array)
        )
        return jax.tree.map(lambda a, b: jnp.where(reached, a, b), new, before)

    return lax.fori_loop(0, size, hop, start)


def head_norm(head_values, gain_vec):
    mean_square = jnp.mean(head_values * head_values, axis=-1, keepdims=True)
    return head_values * lax.rsqrt(mean_square + epsilon) * gain_vec


def decay_factors(gate_preactivation, lower_bound_logit, added_log_decay, number_of_heads):
    token_count = gate_preactivation.shape[0]
    floor_rate = jax.nn.sigmoid(-lower_bound_logit).reshape(number_of_heads, -1)
    state_inflow = floor_rate[None] * jax.nn.sigmoid(
        -gate_preactivation.astype(jnp.float32)
    ).reshape(token_count, number_of_heads, -1)
    decay_logarithm = jnp.log1p(-state_inflow) + added_log_decay[:, :, None]
    return (state_inflow, decay_logarithm)


def recurrence_blocks(queries, decay_logarithm, state_inflow, value_rows, block_len):
    token_count, number_of_heads, key_width = queries.shape
    block_count = token_count // block_len

    def to_blocks(source):
        return source.reshape(block_count, block_len, number_of_heads, source.shape[-1])

    causal = jnp.tril(jnp.ones((block_len, block_len), jnp.float32))[:, :, None, None]

    def block_step(carry_state, inputs):
        query_blk, decay_blk, inflow_blk, value_blk = inputs
        cumulative = jnp.cumsum(decay_blk, axis=0)
        relative = cumulative[:, None] - cumulative[None, :]
        decay_table = jnp.exp(jnp.minimum(relative, 0.0)) * causal
        scores = jnp.einsum(
            "thd,shd,tshd->hts", query_blk, inflow_blk, decay_table, precision=highest
        )
        block_out = jnp.einsum("hts,shv->thv", scores, value_blk, precision=highest)
        block_out = block_out + jnp.einsum(
            "thd,hdv->thv", query_blk * jnp.exp(cumulative), carry_state, precision=highest
        )
        last_log = cumulative[-1]
        new_state = jnp.exp(last_log)[:, :, None] * carry_state + jnp.einsum(
            "shd,shv->hdv",
            inflow_blk * jnp.exp(last_log[None] - cumulative),
            value_blk,
            precision=highest,
        )
        return (new_state, block_out)

    zero_state = jnp.zeros((number_of_heads, key_width, value_rows.shape[-1]), jnp.float32)
    final_state, outputs = lax.scan(
        block_step,
        zero_state,
        (
            to_blocks(queries),
            to_blocks(decay_logarithm),
            to_blocks(state_inflow),
            to_blocks(value_rows),
        ),
    )
    return (final_state, outputs.reshape(token_count, number_of_heads, -1))


def chain_pair(earlier, following):
    return (earlier[0] * following[0], following[0][:, :, None] * earlier[1] + following[1])


def recurrent_path_output(
    recurrent_query,
    recurrent_forget_gate,
    recurrent_value,
    recurrent_gate_lower_bound,
    recurrent_added_decay,
    recurrent_norm_gain,
):
    token_count = recurrent_query.shape[0]
    number_of_heads = recurrent_gate_lower_bound.shape[0] // HG_DK
    state_inflow, decay_logarithm = decay_factors(
        recurrent_forget_gate, recurrent_gate_lower_bound, recurrent_added_decay, number_of_heads
    )
    queries = recurrent_query.astype(jnp.float32).reshape(token_count, number_of_heads, HG_DK)
    value_rows = recurrent_value.astype(jnp.float32).reshape(token_count, number_of_heads, HG_DV)
    final_state, local_out = recurrence_blocks(
        queries, decay_logarithm, state_inflow, value_rows, BLK
    )
    running_log = jnp.cumsum(decay_logarithm, axis=0)
    through = jnp.exp(running_log[-1])
    incoming = carried_in(
        (through, final_state),
        "sp",
        chain_pair,
        (jnp.ones_like(through), jnp.zeros_like(final_state)),
    )
    carried = jnp.einsum(
        "thd,hdv->thv", queries * jnp.exp(running_log), incoming[1], precision=highest
    )
    return (
        head_norm(local_out + carried, recurrent_norm_gain)
        .astype(jnp.bfloat16)
        .reshape(token_count, -1)
    )


def attention_branch(
    attention_query_first,
    attention_key_first,
    attention_query_second,
    attention_key_second,
    attention_value,
    second_map_weight,
    attention_norm_gain,
):
    query_rows = attention_query_first.shape[0]
    key_heads = attention_key_first.shape[1] // DA_HD
    group_size = attention_query_first.shape[1] // DA_HD // key_heads
    score_scale = DA_HD ** (-0.5)
    offset = lax.axis_index("sp") * query_rows
    query_pos = offset + jnp.arange(query_rows)
    last_query = offset + query_rows - 1
    queries_one = attention_query_first.reshape(query_rows, key_heads, group_size, DA_HD)
    queries_two = attention_query_second.reshape(query_rows, key_heads, group_size, DA_HD)

    def map_update(running, queries, key_rows, value_rows, allowed):
        row_max, weight_mass, value_sum = running
        scores = (
            jnp.einsum("qkgd,skd->kgqs", queries, key_rows, preferred_element_type=jnp.float32)
            * score_scale
        )
        scores = jnp.where(allowed, scores, -1e30)
        new_max = jnp.maximum(row_max, jnp.max(scores, axis=-1))
        weights = jnp.where(allowed, jnp.exp(scores - new_max[..., None]), 0.0)
        shrink = jnp.exp(row_max - new_max)
        weight_mass = weight_mass * shrink + jnp.sum(weights, axis=-1)
        value_sum = value_sum * shrink[..., None] + jnp.einsum(
            "plew,wpd->pled",
            weights.astype(jnp.bfloat16),
            value_rows,
            preferred_element_type=jnp.float32,
        )
        return (new_max, weight_mass, value_sum)

    def key_block(running, block_one, block_two, block_values, first_row):
        span_rows = block_one.shape[0]
        key_pos = first_row + jnp.arange(span_rows)
        allowed = key_pos[None, :] <= query_pos[:, None]
        shaped_one = block_one.reshape(span_rows, key_heads, DA_HD)
        shaped_two = block_two.reshape(span_rows, key_heads, DA_HD)
        shaped_values = block_values.reshape(span_rows, key_heads, 2 * DA_HD)
        return (
            map_update(running[0], queries_one, shaped_one, shaped_values, allowed),
            map_update(running[1], queries_two, shaped_two, shaped_values, allowed),
        )

    def guarded_block(running, block_one, block_two, block_values, first_row):

        def compute(state_in):
            return key_block(state_in, block_one, block_two, block_values, first_row)

        def unchanged(state_in):
            return state_in

        result = lax.cond(first_row > last_query, unchanged, compute, running)
        return result

    start_max = jnp.full((key_heads, group_size, query_rows), -1e30, jnp.float32)
    zero_mass = jnp.zeros((key_heads, group_size, query_rows), jnp.float32)
    zero_sum = jnp.zeros((key_heads, group_size, query_rows, 2 * DA_HD), jnp.float32)
    fresh_state = (start_max, zero_mass, zero_sum)
    running = (fresh_state, fresh_state)
    shard_one = lax.all_gather(attention_key_first, "sp", axis=0, tiled=True)
    shard_two = lax.all_gather(attention_key_second, "sp", axis=0, tiled=True)
    shard_values = lax.all_gather(attention_value, "sp", axis=0, tiled=True)
    row_count = shard_one.shape[0]
    span_rows = min(row_count, key_span)
    full_count = row_count // span_rows

    def span_step(span_index, state_in):
        begin_row = span_index * span_rows
        return guarded_block(
            state_in,
            lax.dynamic_slice_in_dim(shard_one, begin_row, span_rows, 0),
            lax.dynamic_slice_in_dim(shard_two, begin_row, span_rows, 0),
            lax.dynamic_slice_in_dim(shard_values, begin_row, span_rows, 0),
            begin_row,
        )

    running = lax.fori_loop(0, full_count, span_step, running)
    first_map, second_map = running
    lambda_table = second_map_weight.reshape(key_heads, group_size)[:, :, None, None]
    combined = first_map[2] / first_map[1][..., None] - lambda_table * (
        second_map[2] / second_map[1][..., None]
    )
    combined = jnp.transpose(combined, (2, 0, 1, 3)).reshape(
        query_rows, key_heads * group_size, 2 * DA_HD
    )
    return head_norm(combined, attention_norm_gain).astype(jnp.bfloat16).reshape(query_rows, -1)


def general_shards(
    recurrent_query,
    recurrent_forget_gate,
    recurrent_value,
    recurrent_gate_lower_bound,
    recurrent_added_decay,
    recurrent_norm_gain,
    attention_query_first,
    attention_key_first,
    attention_query_second,
    attention_key_second,
    attention_value,
    second_map_weight,
    attention_norm_gain,
    output_weight,
):
    attended = attention_branch(
        attention_query_first,
        attention_key_first,
        attention_query_second,
        attention_key_second,
        attention_value,
        second_map_weight,
        attention_norm_gain,
    )
    recurrent_output = recurrent_path_output(
        recurrent_query,
        recurrent_forget_gate,
        recurrent_value,
        recurrent_gate_lower_bound,
        recurrent_added_decay,
        recurrent_norm_gain,
    )
    pieces = lax.all_gather(output_weight, "sp", axis=2, tiled=True)
    partial_terms = jnp.dot(
        recurrent_output, pieces[0], preferred_element_type=jnp.float32
    ) + jnp.dot(attended, pieces[1], preferred_element_type=jnp.float32)
    return lax.psum_scatter(
        partial_terms.astype(jnp.bfloat16), "tp", scatter_dimension=0, tiled=True
    )


f32 = jnp.float32
bf16 = jnp.bfloat16
SPARE_ROWS = 16


PARAMS = pltpu.CompilerParams(vmem_limit_bytes=16 * 1024 * 1024)


def dot_nt(a, b):
    return lax.dot_general(a, b, (((1,), (1,)), ((), ())), preferred_element_type=f32)


def dot_nn(a, b):
    return jnp.dot(a, b, preferred_element_type=f32)


def dot_tn(a, b):
    return lax.dot_general(a, b, (((0,), (0,)), ((), ())), preferred_element_type=f32)


def cost(flops, *arrays):
    moved = sum(a.size * a.dtype.itemsize for a in arrays)
    return pl.CostEstimate(flops=flops, bytes_accessed=moved, transcendentals=0)


BASE = 4 * DA_HD
STATE = slice(BASE, BASE + HG_DV)
FADE = slice(BASE + HG_DV, BASE + HG_DV + SPARE_ROWS)
HBM = pl.BlockSpec(memory_space=pltpu.HBM)
VMEM = pl.BlockSpec(memory_space=pltpu.VMEM)


def prepare_kernel(*refs):
    sources, rest = refs[:13], refs[13:]
    local_ref, faded_ref, packed_ref, front_ref, asked_ref, gain_ref, weight_ref = rest[:7]
    query_ref, gate_ref, value_ref, bound_ref, added_ref, lift_ref, sems = rest[7:]
    token_count, width = query_ref.shape
    heads = width // HG_DK
    chunk = HG_DK
    wide = 2 * DA_HD
    targets = [
        packed_ref.at[:DA_HD, :],
        packed_ref.at[DA_HD:wide, :],
        lift_ref,
        asked_ref.at[:, :wide],
        asked_ref.at[:, wide:],
        gate_ref,
        bound_ref,
        added_ref,
        query_ref,
        value_ref,
        gain_ref.at[0:1, :],
        gain_ref.at[1:2, :],
        weight_ref,
    ]
    copies = [
        pltpu.make_async_copy(source, target, sems.at[k])
        for k, (source, target) in enumerate(zip(sources, targets))
    ]
    for copy in copies[5:] + copies[:5]:
        copy.start()
    for copy in copies[5:8]:
        copy.wait()
    floor_rate = jax.nn.sigmoid(-bound_ref[...])
    inflow = floor_rate * jax.nn.sigmoid(-gate_ref[...].astype(f32))
    log_decay = jnp.log1p(-inflow)
    row = lax.broadcasted_iota(jnp.int32, (chunk, chunk), 0)
    column = lax.broadcasted_iota(jnp.int32, (chunk, chunk), 1)
    causal = row >= column
    lower = jnp.where(causal, 1.0, 0.0).astype(bf16)
    total = jnp.zeros((1, width), f32)
    states = [None] * heads
    for copy in copies[8:]:
        copy.wait()
    for n in range(token_count // chunk):
        rows = slice(n * chunk, (n + 1) * chunk)
        steps = log_decay[rows]
        coarse = steps.astype(bf16)
        fine = (steps - coarse.astype(f32)).astype(bf16)
        extra = []
        for h in range(heads):
            steps_row = jnp.where(causal, added_ref[h : h + 1, rows], 0.0)
            extra.append(
                jnp.broadcast_to(jnp.sum(steps_row, axis=1, keepdims=True), (chunk, HG_DK))
            )
        summed = dot_nn(lower, coarse) + dot_nn(lower, fine) + jnp.concatenate(extra, axis=1)
        final = summed[chunk - 1 : chunk]
        middle = summed[chunk // 2 - 1 : chunk // 2]
        query = query_ref[rows, :].astype(f32)
        inflow_rows = inflow[rows]
        near_query = (query * jnp.exp(summed - middle)).astype(bf16)
        near_key = (inflow_rows * jnp.exp(middle - summed)).astype(bf16)
        tail_key = (inflow_rows * jnp.exp(final - summed)).astype(bf16)
        faded_ref[rows, :] = (query * jnp.exp(summed + total)).astype(bf16)
        if n:
            base_query = (query * jnp.exp(summed)).astype(bf16)
        fade = jnp.exp(final)
        for h in range(heads):
            lanes = slice(h * HG_DK, (h + 1) * HG_DK)
            value = value_ref[rows, lanes]
            scores = dot_nt(near_query[:, lanes], near_key[:, lanes])
            scores = jnp.where(causal, scores, 0.0).astype(bf16)
            out = dot_nn(scores, value)
            grown = dot_tn(value, tail_key[:, lanes])
            if n:
                out = out + dot_nt(base_query[:, lanes], states[h].astype(bf16))
                grown = grown + states[h] * fade[:, lanes]
            states[h] = grown
            local_ref[rows, lanes] = out
        total = total + final
    through = jnp.exp(total)
    for h in range(heads):
        lanes = slice(h * HG_DK, (h + 1) * HG_DK)
        packed_ref[STATE, lanes] = states[h].astype(bf16)
    packed_ref[FADE, :] = jnp.broadcast_to(through, (SPARE_ROWS, width)).astype(bf16)
    for copy in copies[:5]:
        copy.wait()
    for n in range(token_count // wide):
        block = lift_ref[n * wide : (n + 1) * wide, :]
        packed_ref[wide:BASE, n * wide : (n + 1) * wide] = block
    front_ref[:BASE, :] = packed_ref[:BASE, :]
    front_ref[BASE:, :] = asked_ref[...]


def prepare(arrays):
    (
        query,
        gate,
        value,
        bound,
        added,
        gain,
        query_one,
        key_one,
        query_two,
        key_two,
        att_value,
        weight,
        att_gain,
    ) = arrays
    token_count, width = query.shape
    wide = 2 * DA_HD
    rows = BASE + HG_DV + SPARE_ROWS
    shape = jax.ShapeDtypeStruct
    outs = (
        shape((token_count, width), f32),
        shape((token_count, width), bf16),
        shape((rows, width), bf16),
        shape((BASE + token_count, width), bf16),
        shape((token_count, width), bf16),
        shape((2, HG_DV), f32),
        shape((1, weight.shape[0]), f32),
    )
    inputs = (
        key_one.T,
        key_two.T,
        att_value,
        query_one,
        query_two,
        gate,
        bound.reshape(1, -1),
        added.T,
        query,
        value,
        gain.reshape(1, -1),
        att_gain.reshape(1, -1),
        weight.reshape(1, -1),
    )
    return pl.pallas_call(
        prepare_kernel,
        out_shape=outs,
        in_specs=[HBM] * len(inputs),
        out_specs=[VMEM] * len(outs),
        scratch_shapes=[
            pltpu.VMEM((token_count, width), bf16),
            pltpu.VMEM((token_count, width), bf16),
            pltpu.VMEM((token_count, width), bf16),
            pltpu.VMEM((1, width), f32),
            pltpu.VMEM(added.T.shape, f32),
            pltpu.VMEM((token_count, wide), bf16),
            pltpu.SemaphoreType.DMA((len(inputs),)),
        ],
        name="prepare",
        compiler_params=PARAMS,
        cost_estimate=cost(16 * token_count * width * HG_DK, query, gate, value, *outs),
    )(*(pltpu.with_memory_space_constraint(array, pltpu.HBM) for array in inputs))


def normed(values, gain):
    mean_square = jnp.mean(values * values, axis=-1, keepdims=True)
    return (values * lax.rsqrt(mean_square + epsilon) * gain).astype(bf16)


def blend_kernel(own_ref, one_ref, two_ref, out_ref):
    merged = one_ref[STATE, :].astype(f32)
    merged = merged + fade_of(one_ref) * two_ref[STATE, :].astype(f32)
    merged = own_ref[STATE, :].astype(f32) + fade_of(own_ref) * merged
    out_ref[...] = merged.astype(bf16)


def fade_of(ref):
    return ref[BASE + HG_DV : BASE + HG_DV + 1, :].astype(f32)


def blend(own, one, two):
    return pl.pallas_call(
        blend_kernel,
        out_shape=jax.ShapeDtypeStruct((HG_DV, own.shape[1]), bf16),
        name="blend",
        compiler_params=PARAMS,
        cost_estimate=cost(own.size, own, one, two),
    )(own, one, two)


def carry_kernel(local_ref, faded_ref, gain_ref, p1_ref, p2_ref, p3_ref, p4_ref, out_ref):
    heads = local_ref.shape[1] // HG_DV
    place = lax.axis_index("sp")
    merged = p2_ref[STATE, :].astype(f32) + fade_of(p2_ref) * p3_ref[STATE, :].astype(f32)
    incoming = jnp.where(place == 2, merged, p4_ref[...].astype(f32))
    incoming = jnp.where(place == 1, p1_ref[STATE, :].astype(f32), incoming)
    incoming = jnp.where(place == 0, 0.0, incoming).astype(bf16)
    for h in range(heads):
        lanes = slice(h * HG_DV, (h + 1) * HG_DV)
        mixed = local_ref[:, lanes] + dot_nt(faded_ref[:, lanes], incoming[:, lanes])
        out_ref[:, lanes] = normed(mixed, gain_ref[0:1, :])


def carry_in(local, faded, gain, *parts):
    return pl.pallas_call(
        carry_kernel,
        out_shape=jax.ShapeDtypeStruct(local.shape, bf16),
        name="carry",
        compiler_params=PARAMS,
        cost_estimate=cost(4 * local.size * HG_DK, local, faded, *parts),
    )(local, faded, gain, *parts)


def attend(asked, blocks, weight_ref, gain_ref, out_ref):
    wide = 2 * DA_HD
    token_count = asked.shape[0]
    tile = min(token_count, wide)
    lane = lax.broadcasted_iota(jnp.int32, (tile, wide), 1)
    ones = jnp.ones((token_count, wide), bf16)
    valued = []
    for ref, _ in blocks:
        value = [
            ref[wide:BASE, n * wide : (n + 1) * wide] for n in range(token_count // wide)
        ]
        valued.append(jnp.concatenate([jnp.concatenate(value, axis=0), ones], axis=1))
    for t in range(token_count // tile):
        rows = slice(t * tile, (t + 1) * tile)
        row = lax.broadcasted_iota(jnp.int32, (tile, token_count), 0) + t * tile
        column = lax.broadcasted_iota(jnp.int32, (tile, token_count), 1)
        causal = row >= column
        for head in range(2):
            maps = []
            for m in range(2):
                query = asked[rows, m * wide : (m + 1) * wide].astype(f32) * DA_HD ** (-0.5)
                if m != head:
                    query = pltpu.roll(query, DA_HD, 1)
                query = jnp.where((lane < DA_HD) == (m == 0), query, 0.0).astype(bf16)
                scores = []
                for ref, allowed in blocks:
                    score = dot_nn(query, ref[:wide, :])
                    if allowed is None:
                        score = jnp.where(causal, score, -1e30)
                    elif allowed is not True:
                        score = jnp.where(allowed, score, -1e30)
                    scores.append(score)
                top = functools.reduce(jnp.maximum, scores)
                top = jnp.max(top, axis=-1, keepdims=True)
                sums = None
                for part, value in zip(scores, valued):
                    term = dot_nn(jnp.exp(part - top).astype(bf16), value)
                    sums = term if sums is None else sums + term
                maps.append(sums[:, :wide] / sums[:, wide:])
            mixed = maps[0] - weight_ref[0:1, head : head + 1] * maps[1]
            out_ref[rows, head * wide : (head + 1) * wide] = normed(mixed, gain_ref[1:2, :])


def helper_kernel(last, own_ref, p1_ref, p2_ref, p3_ref, weight_ref, gain_ref, out_ref):
    @pl.when(lax.axis_index("sp") == last - 1)
    def _():
        blocks = [(p1_ref, None), (own_ref, True), (p2_ref, True), (p3_ref, True)]
        attend(p1_ref.at[BASE:, :], blocks, weight_ref, gain_ref, out_ref)


def main_kernel(last, asked_ref, own_ref, p1_ref, p2_ref, p3_ref, weight_ref, gain_ref, out_ref):
    place = lax.axis_index("sp")

    @pl.when(place == last - 1)
    def _():
        blocks = [(own_ref, None), (p2_ref, True), (p3_ref, True)]
        attend(asked_ref, blocks, weight_ref, gain_ref, out_ref)

    @pl.when(place < last - 1)
    def _():
        blocks = [(own_ref, None), (p1_ref, place > 0)]
        attend(asked_ref, blocks, weight_ref, gain_ref, out_ref)


def attention(kernel, last, token_count, *arrays):
    width = arrays[0].shape[1]
    return pl.pallas_call(
        functools.partial(kernel, last),
        out_shape=jax.ShapeDtypeStruct((token_count, width), bf16),
        compiler_params=PARAMS,
        cost_estimate=cost(24 * token_count * token_count * width, *arrays),
    )(*arrays)


def project_kernel(flip, tp_size, last, counts, *refs):
    recurrent_refs, main_refs, helped_refs = refs[0:2], refs[2:4], refs[4:6]
    weight_refs, out_ref = list(refs[6:-1]), refs[-1]
    share = recurrent_refs[0].shape[0] // tp_size
    place = lax.axis_index("tp")
    at = lax.axis_index("sp")
    at_end = at == last
    inner = jnp.logical_and(at > 0, at < last)

    def rows_of(pair):
        return jnp.concatenate(
            [
                ref[pl.ds(pl.multiple_of((place ^ flip ^ across) * share, share), share), :]
                for ref in pair
                for across in (0, 2)
            ],
            axis=0,
        )

    recurrent = rows_of(recurrent_refs)
    attended = jnp.where(at_end, rows_of(helped_refs), rows_of(main_refs))
    for p, count in enumerate(counts):
        weight = weight_refs.pop(0)[...]
        if count == 2:
            weight = jnp.where(inner, weight_refs.pop(0)[...], weight)
        width = weight.shape[2]
        terms = dot_nn(recurrent, weight[0]) + dot_nn(attended, weight[1])
        out_ref[:, p * width : (p + 1) * width] = terms.astype(out_ref.dtype)


def project(flip, sizes, mixed, weights, dtype):
    _, sp_size, tp_size = sizes
    rows = 4 * (mixed[0].shape[0] // tp_size)
    counts = tuple(len(w) for w in weights)
    weights = [w for choice in weights for w in choice]
    out = jax.ShapeDtypeStruct((rows, weights[0].shape[2] * len(counts)), dtype)
    return pl.pallas_call(
        functools.partial(project_kernel, flip, tp_size, sp_size - 1, counts),
        out_shape=out,
        name="project",
        compiler_params=PARAMS,
        cost_estimate=cost(4 * rows * mixed[0].shape[1] * out.shape[1], *mixed, *weights, out),
    )(*mixed, *weights)


def pair_kernel(first, kept_ref, came_ref, *out_refs):
    share = out_refs[0].shape[0]
    for k, ref in enumerate(out_refs):
        rows = slice((first + k) * share, (first + k + 1) * share)
        ref[...] = (kept_ref[rows, :] + came_ref[rows, :].astype(f32)).astype(ref.dtype)


def pair_sum(kept, came, first, count, dtype):
    share = (kept.shape[0] // 4, kept.shape[1])
    outs = (jax.ShapeDtypeStruct(share, dtype),) * count
    return pl.pallas_call(
        functools.partial(pair_kernel, first),
        out_shape=outs,
        name="pair",
        compiler_params=PARAMS,
        cost_estimate=cost(kept.size, kept, came, *outs),
    )(kept, came)


def final_kernel(*refs):
    out_ref = refs[-1]
    group = lax.axis_index("grp")
    place = lax.axis_index("sp")
    for n, pieces in enumerate(GROUPS):
        own_ref, across_ref, beside_ref, corner_ref = refs[4 * n : 4 * n + 4]
        width = own_ref.shape[1] // len(pieces)
        for p, d in enumerate(pieces):
            lanes = slice(p * width, (p + 1) * width)
            start = (place ^ d) * (2 * width)
            mine = own_ref[:, lanes] + across_ref[:, lanes].astype(f32)
            theirs = beside_ref[:, lanes].astype(f32) + corner_ref[:, lanes].astype(f32)
            first = pl.multiple_of(start + group * width, width)
            second = pl.multiple_of(start + (1 - group) * width, width)
            out_ref[:, pl.ds(first, width)] = mine.astype(bf16)
            out_ref[:, pl.ds(second, width)] = theirs.astype(bf16)


def final_sum(results):
    arrays = [array for result in results for array in result]
    rows = arrays[0].shape[0]
    width = sum(result[0].shape[1] for result in results)
    out = jax.ShapeDtypeStruct((rows, 2 * width), bf16)
    return pl.pallas_call(
        final_kernel,
        out_shape=out,
        name="final",
        compiler_params=PARAMS,
        cost_estimate=cost(out.size, *arrays, out),
    )(*arrays)


def fast_shards(sizes, *arrays):
    grp_size, sp_size, tp_size = sizes
    output_weight = arrays[13]
    tokens = arrays[0].shape[0]

    def swap(array, axis, size, d):
        return lax.ppermute(array, axis, [(k, k ^ d) for k in range(size)])

    last = sp_size - 1
    local, faded, packed, front, asked, gains, weight = prepare(arrays[:13])
    p0 = lax.ppermute(front, "sp", [(last, 2)])
    p1 = lax.ppermute(packed, "sp", [(0, 1)])
    p2 = lax.ppermute(packed, "sp", [(1, 2)])
    p3 = lax.ppermute(packed, "sp", [(0, 2)])
    half = output_weight.shape[2] // grp_size
    own_weight = lax.dynamic_slice_in_dim(
        output_weight, lax.axis_index("grp") * half, half, axis=2
    )
    weight_one = swap(own_weight, "sp", sp_size, 1)
    weight_mid = lax.ppermute(own_weight, "sp", [(1, 2), (2, 1)])
    weight_far = lax.ppermute(own_weight, "sp", [(0, last), (last, 0)])
    weight_two = lax.ppermute(own_weight, "sp", [(0, 2), (last, 1)])
    weight_end = lax.ppermute(weight_mid, "sp", [(1, 0), (2, last)])
    p4 = lax.ppermute(blend(packed, p2, p3), "sp", [(2, last)])
    helped = attention(helper_kernel, last, tokens, packed, p0, p2, p3, weight, gains)
    helped, asked = lax.optimization_barrier((helped, asked))
    p5 = lax.ppermute(helped, "sp", [(2, last)])
    main = attention(main_kernel, last, tokens, asked, packed, p1, p2, p3, weight, gains)
    recurrent = carry_in(local, faded, gains, p1, p2, p3, p4)
    ends = [
        (g * sp_size + last - 1, (g ^ 1) * sp_size + last) for g in range(grp_size)
    ]
    others = [
        (g * sp_size + k, (g ^ 1) * sp_size + k) for g in range(grp_size) for k in range(last)
    ]
    mixed = (
        recurrent,
        swap(recurrent, "grp", grp_size, 1),
        main,
        lax.ppermute(main, ("grp", "sp"), others),
        p5,
        lax.ppermute(helped, ("grp", "sp"), ends),
    )
    corner_pairs = [
        (g * tp_size + k, (g ^ 1) * tp_size + (k ^ 2))
        for g in range(grp_size)
        for k in range(tp_size)
    ]
    weights = (
        (own_weight,),
        (weight_one,),
        (weight_end, weight_two),
        (weight_far, weight_mid),
    )
    groups = [[weights[d] for d in group] for group in GROUPS]
    results = []
    for weights in groups:
        sent = project(1, sizes, mixed, weights, bf16)
        came = swap(sent, "tp", tp_size, 1)
        kept = project(0, sizes, mixed, weights, f32)
        across, beside, corner = pair_sum(kept, came, 1, 3, bf16)
        (own,) = pair_sum(kept, came, 0, 1, f32)
        across = swap(across, "tp", tp_size, 2)
        beside = swap(beside, "grp", grp_size, 1)
        corner = lax.ppermute(corner, ("grp", "tp"), corner_pairs)
        results.append((own, across, beside, corner))
    return final_sum(results)


GROUPS = ((0, 1, 3), (2,))


def is_short(sizes):
    return sizes == (2, 4, 4)


def shards(sizes, *arrays):
    key_heads = arrays[7].shape[1] // DA_HD
    query_heads = arrays[6].shape[1] // DA_HD
    if is_short(sizes) and key_heads == 1 and query_heads == 2:
        return fast_shards(sizes, *arrays)
    return general_shards(*arrays)


def solution(mesh):
    sizes = (mesh.shape["grp"], mesh.shape["sp"], mesh.shape["tp"])
    return jax.shard_map(
        functools.partial(shards, sizes),
        mesh=mesh,
        in_specs=(
            P(("grp", "sp"), "tp"),
            P(("grp", "sp"), "tp"),
            P(("grp", "sp"), "tp"),
            P("tp"),
            P(("grp", "sp"), "tp"),
            P(),
            P(("grp", "sp"), "tp"),
            P(("grp", "sp"), "tp"),
            P(("grp", "sp"), "tp"),
            P(("grp", "sp"), "tp"),
            P(("grp", "sp"), "tp"),
            P("tp"),
            P(),
            P(None, "tp", "sp"),
        ),
        out_specs=P(("grp", "sp", "tp"), None),
        check_vma=False,
    )
```

```python
import functools

import jax
import jax.numpy as jnp
from jax import lax
from jax.experimental import pallas as pl
from jax.experimental.pallas import tpu as pltpu
from jax.sharding import PartitionSpec as P

HG_DK = 128
HG_DV = 128
DA_HD = 64
BLK = 32


epsilon = 1e-06
highest = lax.Precision.HIGHEST
key_span = 512


def carried_in(array, axis, combine, identity):
    size, place = (lax.axis_size(axis), lax.axis_index(axis))
    everything = jax.tree.map(
        lambda part, kind: lax.all_gather(part.astype(kind), axis),
        array,
        (jnp.bfloat16, jnp.bfloat16),
    )
    start = jax.tree.map(
        lambda part, zero: jnp.broadcast_to(jnp.asarray(zero, part.dtype), part.shape),
        array,
        identity,
    )

    def hop(k, before):
        reached = k < place
        new = combine(
            before, jax.tree.map(lambda part, own: part[k].astype(own.dtype), everything, array)
        )
        return jax.tree.map(lambda a, b: jnp.where(reached, a, b), new, before)

    return lax.fori_loop(0, size, hop, start)


def head_norm(head_values, gain_vec):
    mean_square = jnp.mean(head_values * head_values, axis=-1, keepdims=True)
    return head_values * lax.rsqrt(mean_square + epsilon) * gain_vec


def decay_factors(gate_preactivation, lower_bound_logit, added_log_decay, number_of_heads):
    token_count = gate_preactivation.shape[0]
    floor_rate = jax.nn.sigmoid(-lower_bound_logit).reshape(number_of_heads, -1)
    state_inflow = floor_rate[None] * jax.nn.sigmoid(
        -gate_preactivation.astype(jnp.float32)
    ).reshape(token_count, number_of_heads, -1)
    decay_logarithm = jnp.log1p(-state_inflow) + added_log_decay[:, :, None]
    return (state_inflow, decay_logarithm)


def recurrence_blocks(queries, decay_logarithm, state_inflow, value_rows, block_len):
    token_count, number_of_heads, key_width = queries.shape
    block_count = token_count // block_len

    def to_blocks(source):
        return source.reshape(block_count, block_len, number_of_heads, source.shape[-1])

    causal = jnp.tril(jnp.ones((block_len, block_len), jnp.float32))[:, :, None, None]

    def block_step(carry_state, inputs):
        query_blk, decay_blk, inflow_blk, value_blk = inputs
        cumulative = jnp.cumsum(decay_blk, axis=0)
        relative = cumulative[:, None] - cumulative[None, :]
        decay_table = jnp.exp(jnp.minimum(relative, 0.0)) * causal
        scores = jnp.einsum(
            "thd,shd,tshd->hts", query_blk, inflow_blk, decay_table, precision=highest
        )
        block_out = jnp.einsum("hts,shv->thv", scores, value_blk, precision=highest)
        block_out = block_out + jnp.einsum(
            "thd,hdv->thv", query_blk * jnp.exp(cumulative), carry_state, precision=highest
        )
        last_log = cumulative[-1]
        new_state = jnp.exp(last_log)[:, :, None] * carry_state + jnp.einsum(
            "shd,shv->hdv",
            inflow_blk * jnp.exp(last_log[None] - cumulative),
            value_blk,
            precision=highest,
        )
        return (new_state, block_out)

    zero_state = jnp.zeros((number_of_heads, key_width, value_rows.shape[-1]), jnp.float32)
    final_state, outputs = lax.scan(
        block_step,
        zero_state,
        (
            to_blocks(queries),
            to_blocks(decay_logarithm),
            to_blocks(state_inflow),
            to_blocks(value_rows),
        ),
    )
    return (final_state, outputs.reshape(token_count, number_of_heads, -1))


def chain_pair(earlier, following):
    return (earlier[0] * following[0], following[0][:, :, None] * earlier[1] + following[1])


def recurrent_path_output(
    recurrent_query,
    recurrent_forget_gate,
    recurrent_value,
    recurrent_gate_lower_bound,
    recurrent_added_decay,
    recurrent_norm_gain,
):
    token_count = recurrent_query.shape[0]
    number_of_heads = recurrent_gate_lower_bound.shape[0] // HG_DK
    state_inflow, decay_logarithm = decay_factors(
        recurrent_forget_gate, recurrent_gate_lower_bound, recurrent_added_decay, number_of_heads
    )
    queries = recurrent_query.astype(jnp.float32).reshape(token_count, number_of_heads, HG_DK)
    value_rows = recurrent_value.astype(jnp.float32).reshape(token_count, number_of_heads, HG_DV)
    final_state, local_out = recurrence_blocks(
        queries, decay_logarithm, state_inflow, value_rows, BLK
    )
    running_log = jnp.cumsum(decay_logarithm, axis=0)
    through = jnp.exp(running_log[-1])
    incoming = carried_in(
        (through, final_state),
        "sp",
        chain_pair,
        (jnp.ones_like(through), jnp.zeros_like(final_state)),
    )
    carried = jnp.einsum(
        "thd,hdv->thv", queries * jnp.exp(running_log), incoming[1], precision=highest
    )
    return (
        head_norm(local_out + carried, recurrent_norm_gain)
        .astype(jnp.bfloat16)
        .reshape(token_count, -1)
    )


def attention_branch(
    attention_query_first,
    attention_key_first,
    attention_query_second,
    attention_key_second,
    attention_value,
    second_map_weight,
    attention_norm_gain,
):
    query_rows = attention_query_first.shape[0]
    key_heads = attention_key_first.shape[1] // DA_HD
    group_size = attention_query_first.shape[1] // DA_HD // key_heads
    score_scale = DA_HD ** (-0.5)
    offset = lax.axis_index("sp") * query_rows
    query_pos = offset + jnp.arange(query_rows)
    last_query = offset + query_rows - 1
    queries_one = attention_query_first.reshape(query_rows, key_heads, group_size, DA_HD)
    queries_two = attention_query_second.reshape(query_rows, key_heads, group_size, DA_HD)

    def map_update(running, queries, key_rows, value_rows, allowed):
        row_max, weight_mass, value_sum = running
        scores = (
            jnp.einsum("qkgd,skd->kgqs", queries, key_rows, preferred_element_type=jnp.float32)
            * score_scale
        )
        scores = jnp.where(allowed, scores, -1e30)
        new_max = jnp.maximum(row_max, jnp.max(scores, axis=-1))
        weights = jnp.where(allowed, jnp.exp(scores - new_max[..., None]), 0.0)
        shrink = jnp.exp(row_max - new_max)
        weight_mass = weight_mass * shrink + jnp.sum(weights, axis=-1)
        value_sum = value_sum * shrink[..., None] + jnp.einsum(
            "plew,wpd->pled",
            weights.astype(jnp.bfloat16),
            value_rows,
            preferred_element_type=jnp.float32,
        )
        return (new_max, weight_mass, value_sum)

    def key_block(running, block_one, block_two, block_values, first_row):
        span_rows = block_one.shape[0]
        key_pos = first_row + jnp.arange(span_rows)
        allowed = key_pos[None, :] <= query_pos[:, None]
        shaped_one = block_one.reshape(span_rows, key_heads, DA_HD)
        shaped_two = block_two.reshape(span_rows, key_heads, DA_HD)
        shaped_values = block_values.reshape(span_rows, key_heads, 2 * DA_HD)
        return (
            map_update(running[0], queries_one, shaped_one, shaped_values, allowed),
            map_update(running[1], queries_two, shaped_two, shaped_values, allowed),
        )

    def guarded_block(running, block_one, block_two, block_values, first_row):

        def compute(state_in):
            return key_block(state_in, block_one, block_two, block_values, first_row)

        def unchanged(state_in):
            return state_in

        result = lax.cond(first_row > last_query, unchanged, compute, running)
        return result

    start_max = jnp.full((key_heads, group_size, query_rows), -1e30, jnp.float32)
    zero_mass = jnp.zeros((key_heads, group_size, query_rows), jnp.float32)
    zero_sum = jnp.zeros((key_heads, group_size, query_rows, 2 * DA_HD), jnp.float32)
    fresh_state = (start_max, zero_mass, zero_sum)
    running = (fresh_state, fresh_state)
    shard_one = lax.all_gather(attention_key_first, "sp", axis=0, tiled=True)
    shard_two = lax.all_gather(attention_key_second, "sp", axis=0, tiled=True)
    shard_values = lax.all_gather(attention_value, "sp", axis=0, tiled=True)
    row_count = shard_one.shape[0]
    span_rows = min(row_count, key_span)
    full_count = row_count // span_rows

    def span_step(span_index, state_in):
        begin_row = span_index * span_rows
        return guarded_block(
            state_in,
            lax.dynamic_slice_in_dim(shard_one, begin_row, span_rows, 0),
            lax.dynamic_slice_in_dim(shard_two, begin_row, span_rows, 0),
            lax.dynamic_slice_in_dim(shard_values, begin_row, span_rows, 0),
            begin_row,
        )

    running = lax.fori_loop(0, full_count, span_step, running)
    first_map, second_map = running
    lambda_table = second_map_weight.reshape(key_heads, group_size)[:, :, None, None]
    combined = first_map[2] / first_map[1][..., None] - lambda_table * (
        second_map[2] / second_map[1][..., None]
    )
    combined = jnp.transpose(combined, (2, 0, 1, 3)).reshape(
        query_rows, key_heads * group_size, 2 * DA_HD
    )
    return head_norm(combined, attention_norm_gain).astype(jnp.bfloat16).reshape(query_rows, -1)


def general_shards(
    recurrent_query,
    recurrent_forget_gate,
    recurrent_value,
    recurrent_gate_lower_bound,
    recurrent_added_decay,
    recurrent_norm_gain,
    attention_query_first,
    attention_key_first,
    attention_query_second,
    attention_key_second,
    attention_value,
    second_map_weight,
    attention_norm_gain,
    output_weight,
):
    attended = attention_branch(
        attention_query_first,
        attention_key_first,
        attention_query_second,
        attention_key_second,
        attention_value,
        second_map_weight,
        attention_norm_gain,
    )
    recurrent_output = recurrent_path_output(
        recurrent_query,
        recurrent_forget_gate,
        recurrent_value,
        recurrent_gate_lower_bound,
        recurrent_added_decay,
        recurrent_norm_gain,
    )
    pieces = lax.all_gather(output_weight, "sp", axis=2, tiled=True)
    partial_terms = jnp.dot(
        recurrent_output, pieces[0], preferred_element_type=jnp.float32
    ) + jnp.dot(attended, pieces[1], preferred_element_type=jnp.float32)
    return lax.psum_scatter(
        partial_terms.astype(jnp.bfloat16), "tp", scatter_dimension=0, tiled=True
    )


f32 = jnp.float32
bf16 = jnp.bfloat16
SPARE_ROWS = 16


PARAMS = pltpu.CompilerParams(vmem_limit_bytes=16 * 1024 * 1024)


def dot_nt(a, b):
    return lax.dot_general(a, b, (((1,), (1,)), ((), ())), preferred_element_type=f32)


def dot_nn(a, b):
    return jnp.dot(a, b, preferred_element_type=f32)


def dot_tn(a, b):
    return lax.dot_general(a, b, (((0,), (0,)), ((), ())), preferred_element_type=f32)


def cost(flops, *arrays):
    moved = sum(a.size * a.dtype.itemsize for a in arrays)
    return pl.CostEstimate(flops=flops, bytes_accessed=moved, transcendentals=0)


BASE = 4 * DA_HD
STATE = slice(BASE, BASE + HG_DV)
FADE = slice(BASE + HG_DV, BASE + HG_DV + SPARE_ROWS)
HBM = pl.BlockSpec(memory_space=pltpu.HBM)
VMEM = pl.BlockSpec(memory_space=pltpu.VMEM)


def prepare_kernel(*refs):
    sources, rest = refs[:13], refs[13:]
    local_ref, faded_ref, packed_ref, front_ref, asked_ref, gain_ref, weight_ref = rest[:7]
    query_ref, gate_ref, value_ref, bound_ref, added_ref, lift_ref, sems = rest[7:]
    token_count, width = query_ref.shape
    heads = width // HG_DK
    chunk = HG_DK
    wide = 2 * DA_HD
    targets = [
        packed_ref.at[:DA_HD, :],
        packed_ref.at[DA_HD:wide, :],
        lift_ref,
        asked_ref.at[:, :wide],
        asked_ref.at[:, wide:],
        gate_ref,
        bound_ref,
        added_ref,
        query_ref,
        value_ref,
        gain_ref.at[0:1, :],
        gain_ref.at[1:2, :],
        weight_ref,
    ]
    copies = [
        pltpu.make_async_copy(source, target, sems.at[k])
        for k, (source, target) in enumerate(zip(sources, targets))
    ]
    for copy in copies[5:] + copies[:5]:
        copy.start()
    for copy in copies[5:8]:
        copy.wait()
    floor_rate = jax.nn.sigmoid(-bound_ref[...])
    inflow = floor_rate * jax.nn.sigmoid(-gate_ref[...].astype(f32))
    log_decay = jnp.log1p(-inflow)
    row = lax.broadcasted_iota(jnp.int32, (chunk, chunk), 0)
    column = lax.broadcasted_iota(jnp.int32, (chunk, chunk), 1)
    causal = row >= column
    lower = jnp.where(causal, 1.0, 0.0).astype(bf16)
    total = jnp.zeros((1, width), f32)
    states = [None] * heads
    for copy in copies[8:]:
        copy.wait()
    for n in range(token_count // chunk):
        rows = slice(n * chunk, (n + 1) * chunk)
        steps = log_decay[rows]
        coarse = steps.astype(bf16)
        fine = (steps - coarse.astype(f32)).astype(bf16)
        extra = []
        for h in range(heads):
            steps_row = jnp.where(causal, added_ref[h : h + 1, rows], 0.0)
            extra.append(
                jnp.broadcast_to(jnp.sum(steps_row, axis=1, keepdims=True), (chunk, HG_DK))
            )
        summed = dot_nn(lower, coarse) + dot_nn(lower, fine) + jnp.concatenate(extra, axis=1)
        final = summed[chunk - 1 : chunk]
        middle = summed[chunk // 2 - 1 : chunk // 2]
        query = query_ref[rows, :].astype(f32)
        inflow_rows = inflow[rows]
        near_query = (query * jnp.exp(summed - middle)).astype(bf16)
        near_key = (inflow_rows * jnp.exp(middle - summed)).astype(bf16)
        tail_key = (inflow_rows * jnp.exp(final - summed)).astype(bf16)
        faded_ref[rows, :] = (query * jnp.exp(summed + total)).astype(bf16)
        if n:
            base_query = (query * jnp.exp(summed)).astype(bf16)
        fade = jnp.exp(final)
        for h in range(heads):
            lanes = slice(h * HG_DK, (h + 1) * HG_DK)
            value = value_ref[rows, lanes]
            scores = dot_nt(near_query[:, lanes], near_key[:, lanes])
            scores = jnp.where(causal, scores, 0.0).astype(bf16)
            out = dot_nn(scores, value)
            grown = dot_tn(value, tail_key[:, lanes])
            if n:
                out = out + dot_nt(base_query[:, lanes], states[h].astype(bf16))
                grown = grown + states[h] * fade[:, lanes]
            states[h] = grown
            local_ref[rows, lanes] = out
        total = total + final
    through = jnp.exp(total)
    for h in range(heads):
        lanes = slice(h * HG_DK, (h + 1) * HG_DK)
        packed_ref[STATE, lanes] = states[h].astype(bf16)
    packed_ref[FADE, :] = jnp.broadcast_to(through, (SPARE_ROWS, width)).astype(bf16)
    for copy in copies[:5]:
        copy.wait()
    for n in range(token_count // wide):
        block = lift_ref[n * wide : (n + 1) * wide, :]
        packed_ref[wide:BASE, n * wide : (n + 1) * wide] = block
    front_ref[:BASE, :] = packed_ref[:BASE, :]
    front_ref[BASE:, :] = asked_ref[...]


def prepare(arrays):
    (
        query,
        gate,
        value,
        bound,
        added,
        gain,
        query_one,
        key_one,
        query_two,
        key_two,
        att_value,
        weight,
        att_gain,
    ) = arrays
    token_count, width = query.shape
    wide = 2 * DA_HD
    rows = BASE + HG_DV + SPARE_ROWS
    shape = jax.ShapeDtypeStruct
    outs = (
        shape((token_count, width), f32),
        shape((token_count, width), bf16),
        shape((rows, width), bf16),
        shape((BASE + token_count, width), bf16),
        shape((token_count, width), bf16),
        shape((2, HG_DV), f32),
        shape((1, weight.shape[0]), f32),
    )
    inputs = (
        key_one.T,
        key_two.T,
        att_value,
        query_one,
        query_two,
        gate,
        bound.reshape(1, -1),
        added.T,
        query,
        value,
        gain.reshape(1, -1),
        att_gain.reshape(1, -1),
        weight.reshape(1, -1),
    )
    return pl.pallas_call(
        prepare_kernel,
        out_shape=outs,
        in_specs=[HBM] * len(inputs),
        out_specs=[VMEM] * len(outs),
        scratch_shapes=[
            pltpu.VMEM((token_count, width), bf16),
            pltpu.VMEM((token_count, width), bf16),
            pltpu.VMEM((token_count, width), bf16),
            pltpu.VMEM((1, width), f32),
            pltpu.VMEM(added.T.shape, f32),
            pltpu.VMEM((token_count, wide), bf16),
            pltpu.SemaphoreType.DMA((len(inputs),)),
        ],
        name="prepare",
        compiler_params=PARAMS,
        cost_estimate=cost(16 * token_count * width * HG_DK, query, gate, value, *outs),
    )(*(pltpu.with_memory_space_constraint(array, pltpu.HBM) for array in inputs))


def normed(values, gain):
    mean_square = jnp.mean(values * values, axis=-1, keepdims=True)
    return (values * lax.rsqrt(mean_square + epsilon) * gain).astype(bf16)


def blend_kernel(own_ref, one_ref, two_ref, out_ref):
    merged = one_ref[STATE, :].astype(f32)
    merged = merged + fade_of(one_ref) * two_ref[STATE, :].astype(f32)
    merged = own_ref[STATE, :].astype(f32) + fade_of(own_ref) * merged
    out_ref[...] = merged.astype(bf16)


def fade_of(ref):
    return ref[BASE + HG_DV : BASE + HG_DV + 1, :].astype(f32)


def blend(own, one, two):
    return pl.pallas_call(
        blend_kernel,
        out_shape=jax.ShapeDtypeStruct((HG_DV, own.shape[1]), bf16),
        name="blend",
        compiler_params=PARAMS,
        cost_estimate=cost(own.size, own, one, two),
    )(own, one, two)


def carry_kernel(local_ref, faded_ref, gain_ref, p1_ref, p2_ref, p3_ref, p4_ref, out_ref):
    heads = local_ref.shape[1] // HG_DV
    place = lax.axis_index("sp")
    merged = p2_ref[STATE, :].astype(f32) + fade_of(p2_ref) * p3_ref[STATE, :].astype(f32)
    incoming = jnp.where(place == 2, merged, p4_ref[...].astype(f32))
    incoming = jnp.where(place == 1, p1_ref[STATE, :].astype(f32), incoming)
    incoming = jnp.where(place == 0, 0.0, incoming).astype(bf16)
    for h in range(heads):
        lanes = slice(h * HG_DV, (h + 1) * HG_DV)
        mixed = local_ref[:, lanes] + dot_nt(faded_ref[:, lanes], incoming[:, lanes])
        out_ref[:, lanes] = normed(mixed, gain_ref[0:1, :])


def carry_in(local, faded, gain, *parts):
    return pl.pallas_call(
        carry_kernel,
        out_shape=jax.ShapeDtypeStruct(local.shape, bf16),
        name="carry",
        compiler_params=PARAMS,
        cost_estimate=cost(4 * local.size * HG_DK, local, faded, *parts),
    )(local, faded, gain, *parts)


def attend(asked, blocks, weight_ref, gain_ref, out_ref):
    wide = 2 * DA_HD
    token_count = asked.shape[0]
    tile = min(token_count, wide)
    lane = lax.broadcasted_iota(jnp.int32, (tile, wide), 1)
    ones = jnp.ones((token_count, wide), bf16)
    valued = []
    for ref, _ in blocks:
        value = [
            ref[wide:BASE, n * wide : (n + 1) * wide] for n in range(token_count // wide)
        ]
        valued.append(jnp.concatenate([jnp.concatenate(value, axis=0), ones], axis=1))
    for t in range(token_count // tile):
        rows = slice(t * tile, (t + 1) * tile)
        row = lax.broadcasted_iota(jnp.int32, (tile, token_count), 0) + t * tile
        column = lax.broadcasted_iota(jnp.int32, (tile, token_count), 1)
        causal = row >= column
        for head in range(2):
            maps = []
            for m in range(2):
                query = asked[rows, m * wide : (m + 1) * wide].astype(f32) * DA_HD ** (-0.5)
                if m != head:
                    query = pltpu.roll(query, DA_HD, 1)
                query = jnp.where((lane < DA_HD) == (m == 0), query, 0.0).astype(bf16)
                scores = []
                for ref, allowed in blocks:
                    score = dot_nn(query, ref[:wide, :])
                    if allowed is None:
                        score = jnp.where(causal, score, -1e30)
                    elif allowed is not True:
                        score = jnp.where(allowed, score, -1e30)
                    scores.append(score)
                top = functools.reduce(jnp.maximum, scores)
                top = jnp.max(top, axis=-1, keepdims=True)
                sums = None
                for part, value in zip(scores, valued):
                    term = dot_nn(jnp.exp(part - top).astype(bf16), value)
                    sums = term if sums is None else sums + term
                maps.append(sums[:, :wide] / sums[:, wide:])
            mixed = maps[0] - weight_ref[0:1, head : head + 1] * maps[1]
            out_ref[rows, head * wide : (head + 1) * wide] = normed(mixed, gain_ref[1:2, :])


def helper_kernel(last, own_ref, p1_ref, p2_ref, p3_ref, weight_ref, gain_ref, out_ref):
    @pl.when(lax.axis_index("sp") == last - 1)
    def _():
        blocks = [(p1_ref, None), (own_ref, True), (p2_ref, True), (p3_ref, True)]
        attend(p1_ref.at[BASE:, :], blocks, weight_ref, gain_ref, out_ref)


def main_kernel(last, asked_ref, own_ref, p1_ref, p2_ref, p3_ref, weight_ref, gain_ref, out_ref):
    place = lax.axis_index("sp")

    @pl.when(place == last - 1)
    def _():
        blocks = [(own_ref, None), (p2_ref, True), (p3_ref, True)]
        attend(asked_ref, blocks, weight_ref, gain_ref, out_ref)

    @pl.when(place < last - 1)
    def _():
        blocks = [(own_ref, None), (p1_ref, place > 0)]
        attend(asked_ref, blocks, weight_ref, gain_ref, out_ref)


def attention(kernel, last, token_count, *arrays):
    width = arrays[0].shape[1]
    return pl.pallas_call(
        functools.partial(kernel, last),
        out_shape=jax.ShapeDtypeStruct((token_count, width), bf16),
        compiler_params=PARAMS,
        cost_estimate=cost(24 * token_count * token_count * width, *arrays),
    )(*arrays)


def project_kernel(flip, tp_size, last, counts, *refs):
    recurrent_refs, main_refs, helped_refs = refs[0:2], refs[2:4], refs[4:6]
    weight_refs, out_ref = list(refs[6:-1]), refs[-1]
    share = recurrent_refs[0].shape[0] // tp_size
    place = lax.axis_index("tp")
    at = lax.axis_index("sp")
    at_end = at == last
    inner = jnp.logical_and(at > 0, at < last)

    def rows_of(pair):
        return jnp.concatenate(
            [
                ref[pl.ds(pl.multiple_of((place ^ flip ^ across) * share, share), share), :]
                for ref in pair
                for across in (0, 2)
            ],
            axis=0,
        )

    recurrent = rows_of(recurrent_refs)
    attended = jnp.where(at_end, rows_of(helped_refs), rows_of(main_refs))
    for p, count in enumerate(counts):
        weight = weight_refs.pop(0)[...]
        if count == 2:
            weight = jnp.where(inner, weight_refs.pop(0)[...], weight)
        width = weight.shape[2]
        terms = dot_nn(recurrent, weight[0]) + dot_nn(attended, weight[1])
        out_ref[:, p * width : (p + 1) * width] = terms.astype(out_ref.dtype)


def project(flip, sizes, mixed, weights, dtype):
    _, sp_size, tp_size = sizes
    rows = 4 * (mixed[0].shape[0] // tp_size)
    counts = tuple(len(w) for w in weights)
    weights = [w for choice in weights for w in choice]
    out = jax.ShapeDtypeStruct((rows, weights[0].shape[2] * len(counts)), dtype)
    return pl.pallas_call(
        functools.partial(project_kernel, flip, tp_size, sp_size - 1, counts),
        out_shape=out,
        name="project",
        compiler_params=PARAMS,
        cost_estimate=cost(4 * rows * mixed[0].shape[1] * out.shape[1], *mixed, *weights, out),
    )(*mixed, *weights)


def pair_kernel(first, kept_ref, came_ref, *out_refs):
    share = out_refs[0].shape[0]
    for k, ref in enumerate(out_refs):
        rows = slice((first + k) * share, (first + k + 1) * share)
        ref[...] = (kept_ref[rows, :] + came_ref[rows, :].astype(f32)).astype(ref.dtype)


def pair_sum(kept, came, first, count, dtype):
    share = (kept.shape[0] // 4, kept.shape[1])
    outs = (jax.ShapeDtypeStruct(share, dtype),) * count
    return pl.pallas_call(
        functools.partial(pair_kernel, first),
        out_shape=outs,
        name="pair",
        compiler_params=PARAMS,
        cost_estimate=cost(kept.size, kept, came, *outs),
    )(kept, came)


def final_kernel(*refs):
    out_ref = refs[-1]
    group = lax.axis_index("grp")
    place = lax.axis_index("sp")
    for n, pieces in enumerate(GROUPS):
        own_ref, across_ref, beside_ref, corner_ref = refs[4 * n : 4 * n + 4]
        width = own_ref.shape[1] // len(pieces)
        for p, d in enumerate(pieces):
            lanes = slice(p * width, (p + 1) * width)
            start = (place ^ d) * (2 * width)
            mine = own_ref[:, lanes] + across_ref[:, lanes].astype(f32)
            theirs = beside_ref[:, lanes].astype(f32) + corner_ref[:, lanes].astype(f32)
            first = pl.multiple_of(start + group * width, width)
            second = pl.multiple_of(start + (1 - group) * width, width)
            out_ref[:, pl.ds(first, width)] = mine.astype(bf16)
            out_ref[:, pl.ds(second, width)] = theirs.astype(bf16)


def final_sum(results):
    arrays = [array for result in results for array in result]
    rows = arrays[0].shape[0]
    width = sum(result[0].shape[1] for result in results)
    out = jax.ShapeDtypeStruct((rows, 2 * width), bf16)
    return pl.pallas_call(
        final_kernel,
        out_shape=out,
        name="final",
        compiler_params=PARAMS,
        cost_estimate=cost(out.size, *arrays, out),
    )(*arrays)


def fast_shards(sizes, *arrays):
    grp_size, sp_size, tp_size = sizes
    output_weight = arrays[13]
    tokens = arrays[0].shape[0]

    def swap(array, axis, size, d):
        return lax.ppermute(array, axis, [(k, k ^ d) for k in range(size)])

    last = sp_size - 1
    local, faded, packed, front, asked, gains, weight = prepare(arrays[:13])
    p0 = lax.ppermute(front, "sp", [(last, 2)])
    p1 = lax.ppermute(packed, "sp", [(0, 1)])
    p2 = lax.ppermute(packed, "sp", [(1, 2)])
    p3 = lax.ppermute(packed, "sp", [(0, 2)])
    half = output_weight.shape[2] // grp_size
    own_weight = lax.dynamic_slice_in_dim(
        output_weight, lax.axis_index("grp") * half, half, axis=2
    )
    weight_one = swap(own_weight, "sp", sp_size, 1)
    weight_mid = lax.ppermute(own_weight, "sp", [(1, 2), (2, 1)])
    weight_far = lax.ppermute(own_weight, "sp", [(0, last), (last, 0)])
    weight_two = lax.ppermute(weight_one, "sp", [(1, 2), (2, 1)])
    weight_end = lax.ppermute(weight_mid, "sp", [(1, 0), (2, last)])
    p4 = lax.ppermute(blend(packed, p2, p3), "sp", [(2, last)])
    helped = attention(helper_kernel, last, tokens, packed, p0, p2, p3, weight, gains)
    helped, asked = lax.optimization_barrier((helped, asked))
    p5 = lax.ppermute(helped, "sp", [(2, last)])
    recurrent = carry_in(local, faded, gains, p1, p2, p3, p4)
    recurrent, asked = lax.optimization_barrier((recurrent, asked))
    main = attention(main_kernel, last, tokens, asked, packed, p1, p2, p3, weight, gains)
    ends = [
        (g * sp_size + last - 1, (g ^ 1) * sp_size + last) for g in range(grp_size)
    ]
    mixed = (
        recurrent,
        swap(recurrent, "grp", grp_size, 1),
        main,
        swap(main, "grp", grp_size, 1),
        p5,
        lax.ppermute(helped, ("grp", "sp"), ends),
    )
    corner_pairs = [
        (g * tp_size + k, (g ^ 1) * tp_size + (k ^ 2))
        for g in range(grp_size)
        for k in range(tp_size)
    ]
    weights = (
        (own_weight,),
        (weight_one,),
        (weight_end, weight_two),
        (weight_far, weight_mid),
    )
    groups = [[weights[d] for d in group] for group in GROUPS]
    results = []
    for weights in groups:
        sent = project(1, sizes, mixed, weights, bf16)
        came = swap(sent, "tp", tp_size, 1)
        kept = project(0, sizes, mixed, weights, f32)
        across, beside, corner = pair_sum(kept, came, 1, 3, bf16)
        (own,) = pair_sum(kept, came, 0, 1, f32)
        across = swap(across, "tp", tp_size, 2)
        beside = swap(beside, "grp", grp_size, 1)
        corner = lax.ppermute(corner, ("grp", "tp"), corner_pairs)
        results.append((own, across, beside, corner))
    return final_sum(results)


GROUPS = ((0, 1, 3), (2,))


def is_short(sizes):
    return sizes == (2, 4, 4)


def shards(sizes, *arrays):
    key_heads = arrays[7].shape[1] // DA_HD
    query_heads = arrays[6].shape[1] // DA_HD
    if is_short(sizes) and key_heads == 1 and query_heads == 2:
        return fast_shards(sizes, *arrays)
    return general_shards(*arrays)


def solution(mesh):
    sizes = (mesh.shape["grp"], mesh.shape["sp"], mesh.shape["tp"])
    return jax.shard_map(
        functools.partial(shards, sizes),
        mesh=mesh,
        in_specs=(
            P(("grp", "sp"), "tp"),
            P(("grp", "sp"), "tp"),
            P(("grp", "sp"), "tp"),
            P("tp"),
            P(("grp", "sp"), "tp"),
            P(),
            P(("grp", "sp"), "tp"),
            P(("grp", "sp"), "tp"),
            P(("grp", "sp"), "tp"),
            P(("grp", "sp"), "tp"),
            P(("grp", "sp"), "tp"),
            P("tp"),
            P(),
            P(None, "tp", "sp"),
        ),
        out_specs=P(("grp", "sp", "tp"), None),
        check_vma=False,
    )
```
